32 devices in a mesh: grp: 2 (over y), fs: 4 (over z), tp: 4 (over x, core).
Axes of the slice: x: 2, y: 2, z: 4, core: 2. Of those that a mesh axis runs over, the one named last changes fastest.
Arguments:
- stream: bfloat16 [2048, 3072], P('tp', ('grp', 'fs')), parts along dimension 1, may hold values from -6 to 6
- first_gain: float32 [2048], replicated, may hold values from 0.1 to 1.9
- first_gate: float32 [2048, 5632], P('fs', 'tp'), may hold values from -0.125 to 0.125
- first_gate_scale: float32 [5632], P('tp'), may hold values from 0.5 to 2
- first_up: float32 [2048, 5632], P('fs', 'tp'), may hold values from -0.125 to 0.125
- first_up_scale: float32 [5632], P('tp'), may hold values from 0.5 to 2
- first_down: float32 [5632, 2048], P('tp', 'fs'), may hold values from -0.078125 to 0.078125
- first_down_scale: float32 [2048], P('fs'), may hold values from 0.5 to 2
- mixer_gain: float32 [2048], replicated, may hold values from 0.1 to 1.9
- mixer_left: float32 [2048, 1024], P('fs', 'tp'), may hold values from -0.125 to 0.125
- mixer_left_scale: float32 [1024], P('tp'), may hold values from 0.5 to 2
- mixer_right: float32 [2048, 1024], P('fs', 'tp'), may hold values from -0.125 to 0.125
- mixer_right_scale: float32 [1024], P('tp'), may hold values from 0.5 to 2
- channel_gain: float32 [1024], P('tp'), may hold values from 0.1 to 1.9
- spatial: bfloat16 [8, 128, 128], P('tp'), may hold values from -0.5 to 0.5
- spatial_bias: float32 [8, 128], P('tp'), may hold values from 0.1 to 1.9
- mixer_out: float32 [1024, 2048], P('tp', 'fs'), may hold values from -0.1875 to 0.1875
- mixer_out_scale: float32 [2048], P('fs'), may hold values from 0.5 to 2
- second_gain: float32 [2048], replicated, may hold values from 0.1 to 1.9
- second_gate: float32 [2048, 5632], P('fs', 'tp'), may hold values from -0.125 to 0.125
- second_gate_scale: float32 [5632], P('tp'), may hold values from 0.5 to 2
- second_up: float32 [2048, 5632], P('fs', 'tp'), may hold values from -0.125 to 0.125
- second_up_scale: float32 [5632], P('tp'), may hold values from 0.5 to 2
- second_down: float32 [5632, 2048], P('tp', 'fs'), may hold values from -0.078125 to 0.078125
- second_down_scale: float32 [2048], P('fs'), may hold values from 0.5 to 2
Outputs:
- result: bfloat16 [2048, 3072], P('tp', ('grp', 'fs')), parts along dimension 1
The draws below stay inside these ranges and needn't reach their ends.
There are 2 independent parts, one for each index of `grp`. The reference program is written for one: setup_inputs(seed, part) draws one part's arguments, and reference() takes and returns one part's arrays. A program takes and returns all parts, laid end to end along the dimension named above; an argument that names none is the same for every part. Nothing has to cross between parts.
All inputs are finite; a program needn't handle non-finite values.
Results may differ from the reference program's by a relative error of at most 0.02.
Values may be sent and summed in bfloat16 or wider, within the bound.
A program may use at most 128 MiB of HBM per device.

```python
import math
import jax
import jax.numpy as jnp
from jax import lax

D = 2048
FF = 5632
BRANCH = 1024
GROUPS = 8
BLOCK = 128
TOKENS = 1536
N_TP = 4


def steps_of(rng, dims, split, least, largest):
    def one(axis_at, shards_of):
        draws = jax.random.uniform(jax.random.fold_in(jax.random.fold_in(rng, 6), axis_at), (shards_of,), jnp.float32, least / len(split), largest / len(split))
        return jnp.repeat(jnp.exp(draws), dims[axis_at] // shards_of).reshape((-1,) + (1,) * (len(dims) - axis_at - 1))

    level = one(*split[0])
    for cut in split[1:]:
        level = level * one(*cut)
    return level


def normal_values(own_key, shape, scale, most, split=(), kind=jnp.bfloat16):
    values = jax.random.normal(own_key, shape, jnp.float32) * scale
    if len(split) > 0:
        values = steps_of(own_key, shape, split, -0.22, 0.18) * values
    return jnp.clip(values, min=-most, max=most).astype(kind)


def setup_inputs(seed: int = 0, part: int = 0) -> dict:
    key_of = jax.random.split(jax.random.key(seed), 26)
    own_keys = jax.random.split(jax.random.fold_in(key_of[25], part), 26)
    return {
        "stream": normal_values(own_keys[0], (D, TOKENS), 1.0, 6.0, ((0, 4), (1, 4))),
        "first_gain": jnp.clip(1.0 + 0.18 * jax.random.normal(key_of[1], (D,), jnp.float32), 0.1, 1.9),
        "first_gate": normal_values(key_of[2], (D, FF), D ** -0.5, 0.125, ((0, 4), (1, 4)), jnp.float32),
        "first_gate_scale": jnp.clip(jnp.exp(math.log(2.0) - 1.3862944 * jax.random.uniform(key_of[3], (FF,), jnp.float32) ** steps_of(key_of[3], (FF,), ((0, 4),), -0.2, 0.2)), 0.5, 2.0),
        "first_up": normal_values(key_of[4], (D, FF), D ** -0.5, 0.125, ((0, 4), (1, 4)), jnp.float32),
        "first_up_scale": jnp.clip(jnp.exp(math.log(2.0) - 1.3862944 * jax.random.uniform(key_of[5], (FF,), jnp.float32) ** steps_of(key_of[5], (FF,), ((0, 4),), -0.2, 0.2)), 0.5, 2.0),
        "first_down": normal_values(key_of[6], (FF, D), FF ** -0.5, 0.078125, ((0, 4), (1, 4)), jnp.float32),
        "first_down_scale": jnp.clip(jnp.exp(math.log(2.0) - 1.3862944 * jax.random.uniform(key_of[7], (D,), jnp.float32) ** steps_of(key_of[7], (D,), ((0, 4),), -0.2, 0.2)), 0.5, 2.0),
        "mixer_gain": jnp.clip(1.0 + 0.18 * jax.random.normal(key_of[8], (D,), jnp.float32), 0.1, 1.9),
        "mixer_left": normal_values(key_of[9], (D, BRANCH), D ** -0.5, 0.125, ((0, 4), (1, 4)), jnp.float32),
        "mixer_left_scale": jnp.clip(jnp.exp(math.log(2.0) - 1.3862944 * jax.random.uniform(key_of[10], (BRANCH,), jnp.float32) ** steps_of(key_of[10], (BRANCH,), ((0, 4),), -0.2, 0.2)), 0.5, 2.0),
        "mixer_right": normal_values(key_of[11], (D, BRANCH), D ** -0.5, 0.125, ((0, 4), (1, 4)), jnp.float32),
        "mixer_right_scale": jnp.clip(jnp.exp(math.log(2.0) - 1.3862944 * jax.random.uniform(key_of[12], (BRANCH,), jnp.float32) ** steps_of(key_of[12], (BRANCH,), ((0, 4),), -0.2, 0.2)), 0.5, 2.0),
        "channel_gain": jnp.clip(1.0 + 0.18 * jax.random.normal(key_of[13], (BRANCH,), jnp.float32), 0.1, 1.9),
        "spatial": normal_values(key_of[14], (GROUPS, BLOCK, BLOCK), BLOCK ** -0.5, 0.5, ((0, 4),)),
        "spatial_bias": jnp.clip(1.0 + 0.18 * jax.random.normal(key_of[15], (GROUPS, BLOCK), jnp.float32), 0.1, 1.9),
        "mixer_out": normal_values(key_of[16], (BRANCH, D), BRANCH ** -0.5, 0.1875, ((0, 4), (1, 4)), jnp.float32),
        "mixer_out_scale": jnp.clip(jnp.exp(math.log(2.0) - 1.3862944 * jax.random.uniform(key_of[17], (D,), jnp.float32) ** steps_of(key_of[17], (D,), ((0, 4),), -0.2, 0.2)), 0.5, 2.0),
        "second_gain": jnp.clip(1.0 + 0.18 * jax.random.normal(key_of[18], (D,), jnp.float32), 0.1, 1.9),
        "second_gate": normal_values(key_of[19], (D, FF), D ** -0.5, 0.125, ((0, 4), (1, 4)), jnp.float32),
        "second_gate_scale": jnp.clip(jnp.exp(math.log(2.0) - 1.3862944 * jax.random.uniform(key_of[20], (FF,), jnp.float32) ** steps_of(key_of[20], (FF,), ((0, 4),), -0.2, 0.2)), 0.5, 2.0),
        "second_up": normal_values(key_of[21], (D, FF), D ** -0.5, 0.125, ((0, 4), (1, 4)), jnp.float32),
        "second_up_scale": jnp.clip(jnp.exp(math.log(2.0) - 1.3862944 * jax.random.uniform(key_of[22], (FF,), jnp.float32) ** steps_of(key_of[22], (FF,), ((0, 4),), -0.2, 0.2)), 0.5, 2.0),
        "second_down": normal_values(key_of[23], (FF, D), FF ** -0.5, 0.078125, ((0, 4), (1, 4)), jnp.float32),
        "second_down_scale": jnp.clip(jnp.exp(math.log(2.0) - 1.3862944 * jax.random.uniform(key_of[24], (D,), jnp.float32) ** steps_of(key_of[24], (D,), ((0, 4),), -0.2, 0.2)), 0.5, 2.0),
    }


EPS = 1e-06

def rms_rows(stream, gain):
    values = stream.astype(jnp.float32)
    inverse = lax.rsqrt(lax.optimization_barrier(jnp.mean(values * values, axis=0)) + EPS)
    return (values * inverse * gain[:, None]).astype(jnp.bfloat16)

def project(weight, scale, inputs):
    product = lax.dot_general(weight.astype(jnp.bfloat16), inputs, (((0,), (0,)), ((), ())), preferred_element_type=jnp.float32)
    return product * scale[:, None]

def block_sum(weight, scale, hidden):
    width = weight.shape[0] // N_TP
    total = jnp.zeros((weight.shape[1], hidden.shape[1]), jnp.float32)
    for index in range(N_TP):
        term = project(weight[index * width:(index + 1) * width], scale, hidden[index * width:(index + 1) * width])
        total = total + lax.optimization_barrier(term.astype(jnp.bfloat16)).astype(jnp.float32)
    return total

def half_step(stream, gain, gate_weight, gate_scale, up_weight, up_scale, down_weight, down_scale):
    normed_rows = rms_rows(stream, gain)
    gate = project(gate_weight, gate_scale, normed_rows)
    upward = project(up_weight, up_scale, normed_rows)
    hidden = (jax.nn.silu(gate) * upward).astype(jnp.bfloat16)
    total = block_sum(down_weight, down_scale, hidden)
    return (stream.astype(jnp.float32) + 0.5 * total).astype(jnp.bfloat16)

def reference(stream, first_gain, first_gate, first_gate_scale, first_up, first_up_scale, first_down, first_down_scale, mixer_gain, mixer_left, mixer_left_scale, mixer_right, mixer_right_scale, channel_gain, spatial, spatial_bias, mixer_out, mixer_out_scale, second_gain, second_gate, second_gate_scale, second_up, second_up_scale, second_down, second_down_scale):
    stream = half_step(stream, first_gain, first_gate, first_gate_scale, first_up, first_up_scale, first_down, first_down_scale)
    normed_rows = rms_rows(stream, mixer_gain)
    left = jax.nn.gelu(project(mixer_left, mixer_left_scale, normed_rows))
    right = jax.nn.gelu(project(mixer_right, mixer_right_scale, normed_rows))
    average = lax.optimization_barrier(jnp.mean(right, axis=0))
    squares = lax.optimization_barrier(jnp.mean(right * right, axis=0))
    inverse = lax.rsqrt(squares - average * average + EPS)
    centred = ((right - average) * inverse * channel_gain[:, None]).astype(jnp.bfloat16)
    blocks = centred.reshape(GROUPS, BRANCH // GROUPS, TOKENS // BLOCK, BLOCK)
    lower = jnp.tril(jnp.ones((BLOCK, BLOCK), dtype=bool))
    masked = jnp.where(lower[None], spatial, jnp.zeros_like(spatial))
    token_mix = jnp.einsum('gts,gcns->gcnt', masked.astype(jnp.float32), blocks.astype(jnp.float32))
    token_mix = token_mix + spatial_bias[:, None, None, :]
    gated = (left * token_mix.reshape(BRANCH, TOKENS)).astype(jnp.bfloat16)
    total = block_sum(mixer_out, mixer_out_scale, gated)
    stream = (stream.astype(jnp.float32) + total).astype(jnp.bfloat16)
    return half_step(stream, second_gain, second_gate, second_gate_scale, second_up, second_up_scale, second_down, second_down_scale)
```

```python
import jax
import jax.numpy as jnp
from jax import lax
from jax.experimental import pallas as pl
from jax.experimental.pallas import tpu as pltpu
from jax.sharding import PartitionSpec as P

EPS = 1e-06
CORES = 2
LANES = 128
CHUNKS = 2
MESH = pl.DeviceIdType.MESH
F32, BF16 = jnp.float32, jnp.bfloat16


def many(count):
    return pltpu.SemaphoreType.DMA((count,))


def kernel(
    stream, gate_1, up_1, down_1, left_w, right_w, out_w, gate_2, up_2, down_2,
    gain_1, gain_m, gain_2, gate_scale_1, up_scale_1, down_scale_1, left_scale, right_scale, out_scale,
    gate_scale_2, up_scale_2, down_scale_2, channel_gain, spatial, spatial_bias,
    result,
    weights, mixer_w, staged, turned, wide_in, tall_in, mixer_in,
    rows_1, rows_m, rows_2, normal, hidden, gated, held, kept, stats,
    core_out, core_out_m, core_in_1, core_in_m, core_in_2,
    chip_out, chip_out_m, chip_in_1, chip_in_m, chip_in_2,
    pair_out, pair_in_1, pair_in_2,
    send_sem, recv_sem, load_sem,
):
    grp, fs, tp = lax.axis_index("grp"), lax.axis_index("fs"), lax.axis_index("tp")
    groups, count, tps = lax.axis_size("grp"), lax.axis_size("fs"), lax.axis_size("tp")
    half = count // 2
    side = fs // half
    partner = lax.rem(fs + half, count)
    near = side * half + (1 - lax.rem(fs, half))
    core, chip = lax.rem(tp, CORES), tp // CORES
    sibling = chip * CORES + (1 - core)
    across = lax.rem(tp + CORES, tps)
    diagonal = lax.rem(sibling + CORES, tps)
    wide, tokens = stream.shape
    share = wide // groups
    tall = hidden.shape[1]
    part = tokens // CHUNKS
    branch = left_w.shape[1]

    to_partner, to_near = {"fs": partner}, {"fs": near}
    to_group = {"grp": 1 - grp}
    to_sibling, to_across, to_diagonal = {"tp": sibling}, {"tp": across}, {"tp": diagonal}
    every = (to_partner, to_near, to_group, to_sibling, to_across, to_diagonal)

    barrier = pltpu.get_barrier_semaphore()
    for device in every:
        pl.semaphore_signal(barrier, inc=1, device_id=device, device_id_type=MESH)

    used = [0, 0]
    pending = []

    def send(source, target, device):
        at = used[0]
        used[0] += 1
        copy = pltpu.make_async_remote_copy(
            src_ref=source,
            dst_ref=target,
            send_sem=send_sem.at[at],
            recv_sem=recv_sem.at[at],
            device_id=device,
            device_id_type=MESH,
        )
        copy.start()
        pending.append(copy)
        return copy

    def sent(copies):
        for copy in copies:
            copy.wait_send()
        pending[:] = [other for other in pending if all(other is not copy for copy in copies)]

    def load(source, target):
        at = used[1]
        used[1] += 1
        copy = pltpu.make_async_copy(source, target, load_sem.at[at])
        copy.start()
        return copy

    def place(source, member):
        return pl.ds(pl.multiple_of((source * groups + member) * share, share), share)

    def of_share(member):
        return pl.ds(pl.multiple_of(member * share, share), share)

    own_side = pl.ds(pl.multiple_of(side * tall, 16), tall)
    other_side = pl.ds(pl.multiple_of((1 - side) * tall, 16), tall)


    def load_rows(weight, member, slot):
        return load(weight.at[of_share(member), :], wide_in.at[slot])

    def load_cols(weight, member):
        return load(weight.at[:, of_share(member)], tall_in)

    def load_mixer(member, slot):
        return [
            load(left_w.at[of_share(member), :], mixer_in.at[slot, 0]),
            load(right_w.at[of_share(member), :], mixer_in.at[slot, 1]),
            load(out_w.at[:, of_share(member)], mixer_in.at[slot, 2]),
        ]

    def turn(slot, scale, target):
        def step(at, carry):
            lanes = pl.ds(pl.multiple_of(at * LANES, LANES), LANES)
            target[lanes, :] = (wide_in[slot, :, lanes] * scale[:, lanes]).T.astype(BF16)
            return carry

        lax.fori_loop(0, wide_in.shape[2] // LANES, step, 0)

    def cast_rows(unit, stage, slot, scale):
        target = turned if stage is None else staged.at[stage]
        turn(slot, scale, target)
        member = 1 - grp if stage is None else grp
        weights[unit, :, place(fs, member)] = target[own_side, :]

    def cast_cols(unit, stage, scale):
        member = 1 - grp if stage is None else grp
        factor = scale[:, of_share(member)]
        weights[unit, :, place(fs, member)] = (tall_in[own_side, :] * factor).astype(BF16)
        if stage is not None:
            staged[stage, 0:tall, :] = (tall_in[other_side, :] * factor).astype(BF16)

    def cast_mixer(slot, member):
        at = fs * groups + member
        mixer_w[at, 0:share, :] = (mixer_in[slot, 0] * left_scale[...]).astype(BF16)
        mixer_w[at, share : 2 * share, :] = (mixer_in[slot, 1] * right_scale[...]).astype(BF16)
        mixer_w[at, 2 * share : 3 * share, :] = (
            mixer_in[slot, 2] * out_scale[:, of_share(member)]
        ).astype(BF16)

    class Unit:
        def __init__(self, slot, source):
            self.slot, self.source = slot, source

        def begin(self):
            mine = self.slot(fs, grp)
            self.first = send(self.source() if self.source else mine, mine, to_partner)
            self.second = send(mine, mine, to_near)

        def relay_first(self):
            self.first.wait_recv()
            got = self.slot(partner, grp)
            self.third = send(got, got, to_near)
            self.swaps = [send(got, got, to_group)]

        def relay_second(self):
            self.second.wait_recv()
            got = self.slot(near, grp)
            self.swaps.append(send(got, got, to_group))

        def relay_third(self):
            self.third.wait_recv()
            got = self.slot(lax.rem(near + half, count), grp)
            self.swaps.append(send(got, got, to_group))

        def complete(self):
            for copy in self.swaps:
                copy.wait_recv()

    def hidden_unit(unit, stage, turns):
        return Unit(
            lambda source, member: weights.at[unit, :, place(source, member)],
            lambda: staged.at[stage, other_side if turns else pl.ds(0, tall), :],
        )

    g1, u1, d1 = hidden_unit(0, 0, True), hidden_unit(1, 1, True), hidden_unit(2, 2, False)
    g2, u2, d2 = hidden_unit(3, 0, True), hidden_unit(4, 1, True), hidden_unit(5, 2, False)
    mixer = Unit(lambda source, member: mixer_w.at[source * groups + member], None)


    def gather_begin(rows, pair):
        def view(at_side, at_tp, at):
            first = at_side * tokens + at * part if pair else at * part
            return rows.at[
                pl.ds(pl.multiple_of(first, part), part),
                pl.ds(pl.multiple_of(at_tp * wide, wide), wide),
            ]

        firsts, chips, cores = [], [], []
        for at in range(CHUNKS):
            mine = view(side, tp, at)
            if pair:
                firsts.append(send(mine, mine, to_partner))
            chips.append(send(mine, mine, to_across))
            cores.append(send(mine, mine, to_sibling))
        return view, firsts, chips, cores

    def gather_end(begun):
        view, firsts, chips, cores = begun
        seconds = []
        for at in range(CHUNKS):
            if firsts:
                firsts[at].wait_recv()
                got = view(1 - side, tp, at)
                seconds.append(send(got, got, to_across))
                cores.append(send(got, got, to_sibling))
            chips[at].wait_recv()
            got = view(side, across, at)
            cores.append(send(got, got, to_sibling))
        for at, copy in enumerate(seconds):
            copy.wait_recv()
            got = view(1 - side, across, at)
            cores.append(send(got, got, to_sibling))
        for copy in cores:
            copy.wait_recv()

    def own_rows(rows, pair):
        first = pl.multiple_of(side * tokens, part) if pair else 0
        rows[pl.ds(first, tokens), pl.ds(pl.multiple_of(tp * wide, wide), wide)] = held[...]

    def norm(rows, gain):
        size = 64

        def step(at, carry):
            here = pl.ds(pl.multiple_of(at * size, size), size)
            values = rows[here, :].astype(F32)
            inverse = lax.rsqrt(jnp.mean(values * values, axis=1, keepdims=True) + EPS)
            normal[here, :] = (values * inverse * gain[...]).astype(BF16)
            return carry

        lax.fori_loop(0, rows.shape[0] // size, step, 0)

    def expand(unit):
        def step(at, carry):
            here = pl.ds(pl.multiple_of(at * tokens, tokens), tokens)
            values = normal[here, :]
            dims = (((1,), (1,)), ((), ()))
            gate = lax.dot_general(values, weights[unit], dims, preferred_element_type=F32)
            upward = lax.dot_general(values, weights[unit + 1], dims, preferred_element_type=F32)
            hidden[here, :] = (gate / (1.0 + jnp.exp(-gate)) * upward).astype(BF16)
            return carry

        lax.fori_loop(0, 2, step, 0)

    def reduce_sums(tiles, product, outs, ins, between):
        core_to, chip_to, pair_to = outs
        core_from, chip_from, pair_from = ins
        firsts, seconds, thirds = {}, {}, {}

        def begin(at):
            for to_chip in range(tps // CORES):
                other = to_chip * CORES + 1 - core
                core_to[at, to_chip] = product(tiles[at][0], other).astype(BF16)
            firsts[at] = send(core_to.at[at], core_from.at[at], to_sibling)
            for to_chip in range(tps // CORES):
                kept[at, to_chip] = product(tiles[at][0], to_chip * CORES + core)

        def chips(at):
            firsts[at].wait_recv()
            away = 1 - chip
            chip_to[at] = (kept[at, away] + core_from[at, away].astype(F32)).astype(BF16)
            seconds[at] = send(chip_to.at[at], chip_from.at[at], to_across)
            kept[at, chip] = kept[at, chip] + core_from[at, chip].astype(F32)

        def pairs(at):
            seconds[at].wait_recv()
            total = kept[at, chip] + chip_from[at].astype(F32)
            if tiles[at][1]:
                pair_to[at] = total.astype(BF16)
                thirds[at] = send(pair_to.at[at], pair_from.at[at], to_partner)
            else:
                kept[at, chip] = total

        for at in range(len(tiles) + 2):
            if at < len(tiles):
                begin(at)
            if 0 <= at - 1 < len(tiles):
                chips(at - 1)
            if 0 <= at - 2 < len(tiles):
                pairs(at - 2)
            between(at)
        own = [at for at in range(len(tiles)) if not tiles[at][1]]
        for order, at in enumerate(own):
            total = kept[at, chip]
            if thirds:
                thirds[order].wait_recv()
                total = total + pair_from[order].astype(F32)
            here = pl.ds(order * part, part)
            factor = 0.5 if thirds else 1.0
            held[here, :] = (held[here, :].astype(F32) + factor * total).astype(BF16)
        return list(firsts.values()) + list(seconds.values()) + list(thirds.values())

    def half_tiles():
        away = [((1 - side) * tokens + at * part, True) for at in range(CHUNKS)]
        return away + [(side * tokens + at * part, False) for at in range(CHUNKS)]

    def down_product(unit):
        def product(first, target):
            values = hidden[pl.ds(pl.multiple_of(first, part), part), :]
            columns = pl.ds(pl.multiple_of(target * wide, wide), wide)
            return jnp.dot(values, weights[unit, :, columns], preferred_element_type=F32)

        return product


    def nothing(at):
        pass

    loads = {"g1": load_rows(gate_1, grp, 0), "u1": load_rows(up_1, grp, 1), "d1": load_cols(down_1, grp)}
    held[...] = stream[...].astype(F32).T.astype(BF16)
    own_rows(rows_1, True)
    pl.semaphore_wait(barrier, len(every))
    begun = gather_begin(rows_1, True)

    loads["g1"].wait()
    cast_rows(0, 0, 0, gate_scale_1)
    g1.begin()
    loads["g1"] = load_rows(gate_1, 1 - grp, 0)
    loads["u1"].wait()
    cast_rows(1, 1, 1, up_scale_1)
    u1.begin()
    loads["u1"] = load_rows(up_1, 1 - grp, 1)
    loads["d1"].wait()
    cast_cols(2, 2, down_scale_1)
    d1.begin()
    loads["d1"] = load_cols(down_1, 1 - grp)
    loads["m"] = load_mixer(grp, 0)
    loads["n"] = load_mixer(1 - grp, 1)
    gather_end(begun)
    g1.relay_first()
    g1.relay_second()
    loads["g1"].wait()
    cast_rows(0, None, 0, gate_scale_1)
    loads["g2"] = load_rows(gate_2, grp, 0)
    u1.relay_first()
    u1.relay_second()
    loads["u1"].wait()
    cast_rows(1, None, 1, up_scale_1)
    loads["u2"] = load_rows(up_2, grp, 1)
    d1.relay_first()
    d1.relay_second()
    loads["d1"].wait()
    cast_cols(2, None, down_scale_1)
    loads["d2"] = load_cols(down_2, grp)
    norm(rows_1, gain_1)
    for copy in loads["m"] + loads["n"]:
        copy.wait()
    cast_mixer(0, grp)
    cast_mixer(1, 1 - grp)
    g1.relay_third()
    sent([g1.first, u1.first, d1.first])
    loads["g2"].wait()
    cast_rows(3, 0, 0, gate_scale_2)
    loads["g2"] = load_rows(gate_2, 1 - grp, 0)
    u1.relay_third()
    loads["u2"].wait()
    cast_rows(4, 1, 1, up_scale_2)
    loads["u2"] = load_rows(up_2, 1 - grp, 1)
    d1.relay_third()
    mixer.begin()
    g1.complete()
    u1.complete()
    expand(0)
    d1.complete()

    def between_1(at):
        if at == 4:
            mixer.relay_first()
            mixer.relay_second()

    copies = reduce_sums(
        half_tiles(), down_product(2), (core_out, chip_out, pair_out),
        (core_in_1, chip_in_1, pair_in_1), between_1,
    )

    own_rows(rows_m, False)
    begun = gather_begin(rows_m, False)
    g2.begin()
    u2.begin()
    mixer.relay_third()
    loads["d2"].wait()
    cast_cols(5, 2, down_scale_2)
    loads["d2"] = load_cols(down_2, 1 - grp)
    gather_end(begun)
    norm(rows_m, gain_m)
    mixer.complete()

    def projection(first):
        total = None
        for at in range(count * groups):
            term = jnp.dot(
                normal[0:tokens, at * share : (at + 1) * share],
                mixer_w[at, first : first + share, :],
                preferred_element_type=F32,
            )
            total = term if total is None else total + term
        return jax.nn.gelu(total)

    right = projection(share)
    lane = lax.broadcasted_iota(jnp.int32, (tokens, LANES), 1)
    sums = jnp.sum(right, axis=1, keepdims=True)
    squares = jnp.sum(right * right, axis=1, keepdims=True)
    packed = jnp.where(lane == 0, sums, jnp.where(lane == 1, squares, 0.0))
    stats[0] = packed.T[0:8, :]
    shared = [
        send(stats.at[0], stats.at[1], to_sibling),
        send(stats.at[0], stats.at[2], to_across),
        send(stats.at[0], stats.at[3], to_diagonal),
    ]
    left = projection(0)
    for copy in shared:
        copy.wait_recv()
    total = (stats[0] + stats[1]) + (stats[2] + stats[3])
    total = jnp.concatenate([total, jnp.zeros((LANES - 8, tokens), F32)], axis=0).T
    size = branch * tps
    average = total[:, 0:1] / size
    inverse = lax.rsqrt(total[:, 1:2] / size - average * average + EPS)
    centred = ((right - average) * inverse * channel_gain[...]).astype(BF16)
    span = spatial.shape[1]
    target = lax.broadcasted_iota(jnp.int32, (span, span), 0)
    source = lax.broadcasted_iota(jnp.int32, (span, span), 1)
    members = branch // spatial.shape[0]
    for group in range(spatial.shape[0]):
        matrix = jnp.where(source <= target, spatial[group].astype(F32), 0.0).astype(BF16)
        columns = slice(group * members, (group + 1) * members)
        for at in range(tokens // span):
            here = slice(at * span, (at + 1) * span)
            mixed = jnp.dot(matrix, centred[here, columns], preferred_element_type=F32)
            mixed = mixed + spatial_bias[:, group : group + 1]
            gated[here, columns] = (left[here, columns] * mixed).astype(BF16)
    g2.relay_first()
    g2.relay_second()

    def out_product(first, target):
        values = gated[first : first + part, :]
        each = wide // share
        return jnp.concatenate(
            [
                jnp.dot(
                    values,
                    mixer_w[target * each + at, 2 * share : 3 * share, :],
                    preferred_element_type=F32,
                )
                for at in range(each)
            ],
            axis=1,
        )

    reduce_sums(
        [(at * part, False) for at in range(CHUNKS)], out_product, (core_out_m, chip_out_m, None),
        (core_in_m, chip_in_m, None), nothing,
    )

    own_rows(rows_2, True)
    begun = gather_begin(rows_2, True)
    d2.begin()
    u2.relay_first()
    u2.relay_second()
    g2.relay_third()
    loads["g2"].wait()
    cast_rows(3, None, 0, gate_scale_2)
    loads["u2"].wait()
    cast_rows(4, None, 1, up_scale_2)
    loads["d2"].wait()
    cast_cols(5, None, down_scale_2)
    gather_end(begun)
    norm(rows_2, gain_2)
    u2.relay_third()
    d2.relay_first()
    d2.relay_second()
    g2.complete()
    u2.complete()
    expand(3)
    d2.relay_third()
    d2.complete()
    sent(copies)
    reduce_sums(
        half_tiles(), down_product(5), (core_out, chip_out, pair_out),
        (core_in_2, chip_in_2, pair_in_2), nothing,
    )
    result[...] = held[...].astype(F32).T.astype(BF16)
    for copy in list(pending):
        copy.wait_send()


def contract(left_side, right_side):
    return lax.dot_general(
        left_side, right_side, (((0,), (0,)), ((), ())), preferred_element_type=jnp.float32
    )


def product(left_side, right_side):
    return lax.dot_general(
        left_side, right_side, (((1,), (0,)), ((), ())), preferred_element_type=jnp.float32
    )


def permuted(block, axis_name, target):
    count = lax.axis_size(axis_name)
    return lax.ppermute(block, axis_name, [(at, target(at, count)) for at in range(count)])


def to_partner(block):
    return permuted(block, "fs", lambda at, count: (at + count // 2) % count)


def in_half(block, step):
    def target(at, count):
        half = count // 2
        return at // half * half + (at % half + step) % half

    return permuted(block, "fs", target)


def to_other_grp(block, step):
    return permuted(block, "grp", lambda at, count: (at + step) % count)


def to_same_core(block, step):
    return permuted(block, "tp", lambda at, count: (at + step * CORES) % count)


def to_other_core(block):
    return permuted(block, "tp", lambda at, count: at ^ 1)


def pick(blocks, index):
    count = len(blocks)
    if count == 1:
        return blocks[0]
    index = lax.rem(index + count, count)
    found = blocks[0]
    for at in range(1, count):
        found = jnp.where(index == at, blocks[at], found)
    return found


def chip_and_core():
    place = lax.axis_index("tp")
    return lax.div(place, CORES), lax.rem(place, CORES)


def gather_rows(block):
    chips = lax.axis_size("tp") // CORES
    chip, core = chip_and_core()
    held = jnp.stack([block] + [to_same_core(block, step) for step in range(1, chips)])
    other = to_other_core(held)
    found = []
    for at_chip in range(chips):
        mine = pick([held[step] for step in range(chips)], chip - at_chip)
        theirs = pick([other[step] for step in range(chips)], chip - at_chip)
        found += [jnp.where(core == 0, mine, theirs), jnp.where(core == 0, theirs, mine)]
    return jnp.concatenate(found)


def scatter_sum(terms):
    chips = lax.axis_size("tp") // CORES
    chip, core = chip_and_core()
    blocks = terms.reshape((chips, CORES, -1) + terms.shape[1:])
    mine = jnp.where(core == 0, blocks[:, 0], blocks[:, 1])
    passed = jnp.where(core == 0, blocks[:, 1], blocks[:, 0])
    pairs = mine.astype(jnp.float32) + to_other_core(passed).astype(jnp.float32)
    total = pick([pairs[at] for at in range(chips)], chip)
    for step in range(1, chips):
        sent = pick([pairs[at] for at in range(chips)], chip + step).astype(jnp.bfloat16)
        total = total + to_same_core(sent, step).astype(jnp.float32)
    return total


def places():
    count = lax.axis_size("fs")
    half = count // 2
    me = lax.axis_index("fs")
    low = lax.rem(me, half)
    found = []
    for step in range(half):
        near = me - low + lax.rem(low - step + half, half)
        found += [near, lax.rem(near + half, count)]
    return found


def shares():
    count = lax.axis_size("grp")
    me = lax.axis_index("grp")
    return [lax.rem(me - back + count, count) for back in range(count)]


def gathered(kept, passed, others):
    half = lax.axis_size("fs") // 2
    got = to_partner(passed)
    mine = [kept, got]
    for step in range(1, half):
        mine += [in_half(kept, step), in_half(got, step)]
    found = [mine]
    for back, own in zip(range(1, lax.axis_size("grp")), others):
        found.append([own] + [to_other_grp(block, back) for block in mine[1:]])
    return found


def rows_unit(weights):
    half = lax.div(lax.axis_index("fs"), lax.axis_size("fs") // 2)

    def cut(index, side):
        found = []
        for weight in weights:
            width = weight.shape[0] // lax.axis_size("grp")
            wide = weight.shape[1] // 2
            part = lax.dynamic_slice(weight, (index * width, side * wide), (width, wide))
            found.append(part.astype(jnp.bfloat16).T)
        return jnp.stack(found)

    order = shares()
    return gathered(
        cut(order[0], half), cut(order[0], 1 - half), [cut(index, half) for index in order[1:]]
    )


def cols_unit(weight):
    half = lax.div(lax.axis_index("fs"), lax.axis_size("fs") // 2)

    def cut(index, side):
        width = weight.shape[1] // lax.axis_size("grp")
        tall = weight.shape[0] // 2
        part = lax.dynamic_slice(weight, (side * tall, index * width), (tall, width))
        return part.astype(jnp.bfloat16)

    order = shares()
    return gathered(
        cut(order[0], half), cut(order[0], 1 - half), [cut(index, half) for index in order[1:]]
    )


def mixer_unit(left, right, out):
    def cut(index):
        width = left.shape[0] // lax.axis_size("grp")
        rows = [
            lax.dynamic_slice_in_dim(weight, index * width, width, 0).astype(jnp.bfloat16).T
            for weight in (left, right)
        ]
        return jnp.stack(rows + [lax.dynamic_slice_in_dim(out, index * width, width, 1).astype(jnp.bfloat16)])

    order = shares()
    share = cut(order[0])
    return gathered(share, share, [cut(index) for index in order[1:]])


def rows_in_order(rows):
    count, groups = lax.axis_size("fs"), lax.axis_size("grp")
    width = rows.shape[0] // (count * groups)
    pieces = []
    for share in shares():
        for place in places():
            pieces.append(
                lax.dynamic_slice_in_dim(rows, (place * groups + share) * width, width, 0)
            )
    return jnp.concatenate(pieces)


def joined(blocks):
    return jnp.concatenate([block for mine in blocks for block in mine], axis=-1)


def columns_out(blocks, hidden):
    count, groups = lax.axis_size("fs"), lax.axis_size("grp")
    every = joined(blocks)
    width = every.shape[1] // (count * groups)
    terms = contract(every, hidden).astype(jnp.bfloat16)
    found = jnp.zeros_like(terms)
    at = 0
    for share in shares():
        for place in places():
            found = lax.dynamic_update_slice_in_dim(
                found, terms[at : at + width], (place * groups + share) * width, 0
            )
            at += width
    return found


def inverse_of(values):
    return lax.rsqrt(jnp.mean(values * values, axis=0) + EPS)


def normed(whole_rows, gain):
    values = whole_rows.astype(jnp.float32)
    return (values * inverse_of(values) * gain[:, None]).astype(jnp.bfloat16)


def half_step(stream, gain, rows_blocks, gate_scale, up_scale, cols_blocks, down_scale):
    tokens = stream.shape[1]
    both = jnp.concatenate([stream, to_partner(stream)], axis=1)
    rows = rows_in_order(normed(gather_rows(both), gain))
    half = lax.div(lax.axis_index("fs"), lax.axis_size("fs") // 2)
    tall = gate_scale.shape[0] // 2
    gate_scale = lax.dynamic_slice_in_dim(gate_scale, half * tall, tall)[:, None]
    up_scale = lax.dynamic_slice_in_dim(up_scale, half * tall, tall)[:, None]
    every = joined(rows_blocks)
    gate = product(every[0], rows)
    upward = product(every[1], rows)
    hidden = (jax.nn.silu(gate * gate_scale) * (upward * up_scale)).astype(jnp.bfloat16)
    total = scatter_sum(columns_out(cols_blocks, hidden))
    away = to_partner(total[:, tokens:].astype(jnp.bfloat16))
    total = total[:, :tokens] + away.astype(jnp.float32)
    return (stream.astype(jnp.float32) + 0.5 * (total * down_scale[:, None])).astype(jnp.bfloat16)


def gating_unit(left_pre, right_pre, channel_gain, spatial, spatial_bias):
    left = jax.nn.gelu(left_pre)
    right = jax.nn.gelu(right_pre)
    branch = channel_gain.shape[0] * lax.axis_size("tp")
    totals, squares = lax.psum((jnp.sum(right, axis=0), jnp.sum(right * right, axis=0)), "tp")
    average = totals / branch
    inverse = lax.rsqrt(squares / branch - average * average + EPS)
    centred = ((right - average) * inverse * channel_gain[:, None]).astype(jnp.bfloat16)
    local_groups, span = (spatial.shape[0], spatial.shape[1])
    tokens = centred.shape[1]
    blocks = centred.reshape(local_groups, centred.shape[0] // local_groups, tokens // span, span)
    target = lax.broadcasted_iota(jnp.int32, (span, span), 0)
    source = lax.broadcasted_iota(jnp.int32, (span, span), 1)
    masked = jnp.where((source <= target)[None], spatial, jnp.zeros_like(spatial))
    token_mix = jnp.einsum("gts,gcns->gcnt", masked, blocks, preferred_element_type=jnp.float32)
    token_mix = token_mix + spatial_bias[:, None, None, :]
    return (left * token_mix.reshape(centred.shape[0], tokens)).astype(jnp.bfloat16)


def layer(
    stream,
    first_gain,
    first_gate,
    first_gate_scale,
    first_up,
    first_up_scale,
    first_down,
    first_down_scale,
    mixer_gain,
    mixer_left,
    mixer_left_scale,
    mixer_right,
    mixer_right_scale,
    channel_gain,
    spatial,
    spatial_bias,
    mixer_out,
    mixer_out_scale,
    second_gain,
    second_gate,
    second_gate_scale,
    second_up,
    second_up_scale,
    second_down,
    second_down_scale,
):
    held = jnp.stack([first_down_scale, mixer_out_scale, second_down_scale])
    count = lax.axis_size("fs")
    me = lax.axis_index("fs")
    parts = [held] + [
        permuted(held, "fs", lambda at, count, step=step: (at + step) % count)
        for step in range(1, count)
    ]
    scales = jnp.concatenate([pick(parts, me - place) for place in range(count)], axis=1)
    wide = stream.shape[0]
    scales = lax.dynamic_slice_in_dim(scales, lax.axis_index("tp") * wide, wide, 1)

    first_rows = rows_unit((first_gate, first_up))
    first_cols = cols_unit(first_down)
    mixer = mixer_unit(mixer_left, mixer_right, mixer_out)
    second_rows = rows_unit((second_gate, second_up))
    second_cols = cols_unit(second_down)

    stream = half_step(
        stream, first_gain, first_rows, first_gate_scale, first_up_scale, first_cols, scales[0]
    )
    rows = rows_in_order(normed(gather_rows(stream), mixer_gain))
    lefts = joined([[block[0] for block in mine] for mine in mixer])
    rights = joined([[block[1] for block in mine] for mine in mixer])
    gated = gating_unit(
        product(lefts, rows) * mixer_left_scale[:, None],
        product(rights, rows) * mixer_right_scale[:, None],
        channel_gain,
        spatial,
        spatial_bias,
    )
    total = scatter_sum(columns_out([[block[2] for block in mine] for mine in mixer], gated))
    stream = (stream.astype(jnp.float32) + total * scales[1][:, None]).astype(jnp.bfloat16)
    return half_step(
        stream, second_gain, second_rows, second_gate_scale, second_up_scale, second_cols, scales[2]
    )


def fits(stream, first_gate, mixer_left):
    groups, count, tps = lax.axis_size("grp"), lax.axis_size("fs"), lax.axis_size("tp")
    share = stream.shape[0] // groups
    tall = first_gate.shape[1] // 2
    return (
        groups == 2
        and count == 4
        and tps == 2 * CORES
        and first_gate.shape[0] == stream.shape[0]
        and share % LANES == 0
        and mixer_left.shape[1] == share
        and tall % 16 == 0
        and (2 * tall) % LANES == 0
        and stream.shape[1] % LANES == 0
    )


def fused(
    stream, first_gain, first_gate, first_gate_scale, first_up, first_up_scale, first_down, first_down_scale,
    mixer_gain, mixer_left, mixer_left_scale, mixer_right, mixer_right_scale, channel_gain, spatial,
    spatial_bias, mixer_out, mixer_out_scale, second_gain, second_gate, second_gate_scale, second_up,
    second_up_scale, second_down, second_down_scale,
):
    def flat(vector):
        return vector.reshape(1, -1)

    groups, count, tps = lax.axis_size("grp"), lax.axis_size("fs"), lax.axis_size("tp")
    wide, tokens = stream.shape
    share, tall, depth = wide // groups, first_gate.shape[1] // 2, wide * tps
    branch, part = mixer_left.shape[1], tokens // CHUNKS
    both = 2 * tokens
    any_spec, vmem = pl.BlockSpec(memory_space=pl.ANY), pl.BlockSpec(memory_space=pltpu.VMEM)
    chips = tps // CORES
    vm = pltpu.VMEM
    call = pl.pallas_call(
        kernel,
        out_shape=jax.ShapeDtypeStruct((wide, tokens), BF16),
        in_specs=[vmem] + [any_spec] * 9 + [vmem] * 15,
        out_specs=vmem,
        scratch_shapes=[
            vm((6, tall, depth), BF16),
            vm((count * groups, 3 * share, branch), BF16),
            vm((3, 2 * tall, share), BF16),
            vm((2 * tall, share), BF16),
            vm((2, share, 2 * tall), F32),
            vm((2 * tall, share), F32),
            vm((2, 3, share, branch), F32),
            vm((both, depth), BF16),
            vm((tokens, depth), BF16),
            vm((both, depth), BF16),
            vm((both, depth), BF16),
            vm((both, tall), BF16),
            vm((tokens, branch), BF16),
            vm((tokens, wide), BF16),
            vm((2 * CHUNKS, chips, part, wide), F32),
            vm((4, 8, tokens), F32),
            vm((2 * CHUNKS, chips, part, wide), BF16),
            vm((CHUNKS, chips, part, wide), BF16),
            vm((2 * CHUNKS, chips, part, wide), BF16),
            vm((CHUNKS, chips, part, wide), BF16),
            vm((2 * CHUNKS, chips, part, wide), BF16),
            vm((2 * CHUNKS, part, wide), BF16),
            vm((CHUNKS, part, wide), BF16),
            vm((2 * CHUNKS, part, wide), BF16),
            vm((CHUNKS, part, wide), BF16),
            vm((2 * CHUNKS, part, wide), BF16),
            vm((CHUNKS, part, wide), BF16),
            vm((CHUNKS, part, wide), BF16),
            vm((CHUNKS, part, wide), BF16),
            many(42 + 17 * CHUNKS + 12 * CHUNKS + 3),
            many(42 + 17 * CHUNKS + 12 * CHUNKS + 3),
            many(18),
        ],
        compiler_params=pltpu.CompilerParams(
            collective_id=0, has_side_effects=True, vmem_limit_bytes=67043328
        ),
    )
    return call(
        stream, first_gate, first_up, first_down, mixer_left, mixer_right, mixer_out,
        second_gate, second_up, second_down, flat(first_gain), flat(mixer_gain), flat(second_gain),
        flat(first_gate_scale), flat(first_up_scale), flat(first_down_scale), flat(mixer_left_scale),
        flat(mixer_right_scale), flat(mixer_out_scale), flat(second_gate_scale), flat(second_up_scale),
        flat(second_down_scale), flat(channel_gain), spatial, spatial_bias.T,
    )


def local(*args):
    if fits(args[0], args[2], args[9]):
        return fused(*args)
    return layer(*args)


def solution(mesh):
    return jax.shard_map(
        local,
        mesh=mesh,
        in_specs=(
            P("tp", ("grp", "fs")),
            P(),
            P("fs", "tp"),
            P("tp"),
            P("fs", "tp"),
            P("tp"),
            P("tp", "fs"),
            P("fs"),
            P(),
            P("fs", "tp"),
            P("tp"),
            P("fs", "tp"),
            P("tp"),
            P("tp"),
            P("tp", None, None),
            P("tp", None),
            P("tp", "fs"),
            P("fs"),
            P(),
            P("fs", "tp"),
            P("tp"),
            P("fs", "tp"),
            P("tp"),
            P("tp", "fs"),
            P("fs"),
        ),
        out_specs=P("tp", ("grp", "fs")),
        check_vma=False,
    )
```

```python
import jax
import jax.numpy as jnp
from jax import lax
from jax.experimental import pallas as pl
from jax.experimental.pallas import tpu as pltpu
from jax.sharding import PartitionSpec as P

EPS = 1e-06
CORES = 2
LANES = 128
CHUNKS = 3
PIECES = 2
MESH = pl.DeviceIdType.MESH
F32, BF16 = jnp.float32, jnp.bfloat16


def many(count):
    return pltpu.SemaphoreType.DMA((count,))


def kernel(
    stream, gate_1, up_1, down_1, left_w, right_w, out_w, gate_2, up_2, down_2,
    gain_1, gain_m, gain_2, gate_scale_1, up_scale_1, down_scale_1, left_scale, right_scale, out_scale,
    gate_scale_2, up_scale_2, down_scale_2, channel_gain, spatial, spatial_bias,
    result,
    weights, mixer_w, staged, turned, wide_in, tall_in, mixer_in,
    rows_1, rows_m, rows_2, normal, hidden, gated, held, kept, stats,
    core_out, core_out_m, core_in_1, core_in_m, core_in_2,
    chip_out, chip_out_m, chip_in_1, chip_in_m, chip_in_2,
    pair_out, pair_in_1, pair_in_2,
    send_sem, recv_sem, load_sem,
):
    grp, fs, tp = lax.axis_index("grp"), lax.axis_index("fs"), lax.axis_index("tp")
    groups, count, tps = lax.axis_size("grp"), lax.axis_size("fs"), lax.axis_size("tp")
    half = count // 2
    side = fs // half
    partner = lax.rem(fs + half, count)
    near = side * half + (1 - lax.rem(fs, half))
    core, chip = lax.rem(tp, CORES), tp // CORES
    sibling = chip * CORES + (1 - core)
    across = lax.rem(tp + CORES, tps)
    diagonal = lax.rem(sibling + CORES, tps)
    wide, tokens = stream.shape
    share = wide // groups
    tall = hidden.shape[1]
    part = tokens // CHUNKS
    branch = left_w.shape[1]

    to_partner, to_near = {"fs": partner}, {"fs": near}
    to_group = {"grp": 1 - grp}
    to_sibling, to_across, to_diagonal = {"tp": sibling}, {"tp": across}, {"tp": diagonal}
    every = (to_partner, to_near, to_group, to_sibling, to_across, to_diagonal)

    barrier = pltpu.get_barrier_semaphore()
    for device in every:
        pl.semaphore_signal(barrier, inc=1, device_id=device, device_id_type=MESH)

    used = [0, 0]
    pending = []

    def send(source, target, device):
        at = used[0]
        used[0] += 1
        copy = pltpu.make_async_remote_copy(
            src_ref=source,
            dst_ref=target,
            send_sem=send_sem.at[at],
            recv_sem=recv_sem.at[at],
            device_id=device,
            device_id_type=MESH,
        )
        copy.start()
        pending.append(copy)
        return copy

    def reserve(source, target, device):
        at = used[0]
        used[0] += 1
        return pltpu.make_async_remote_copy(
            src_ref=source,
            dst_ref=target,
            send_sem=send_sem.at[at],
            recv_sem=recv_sem.at[at],
            device_id=device,
            device_id_type=MESH,
        )

    def sent(copies):
        for copy in copies:
            copy.wait_send()
        pending[:] = [other for other in pending if all(other is not copy for copy in copies)]

    def load(source, target):
        at = used[1]
        used[1] += 1
        copy = pltpu.make_async_copy(source, target, load_sem.at[at])
        copy.start()
        return copy

    def place(source, member):
        return pl.ds(pl.multiple_of((source * groups + member) * share, share), share)

    def of_share(member):
        return pl.ds(pl.multiple_of(member * share, share), share)

    own_side = pl.ds(pl.multiple_of(side * tall, 16), tall)
    other_side = pl.ds(pl.multiple_of((1 - side) * tall, 16), tall)


    def load_rows(weight, member, slot):
        return load(weight.at[of_share(member), :], wide_in.at[slot])

    def load_cols(weight, member):
        return load(weight.at[:, of_share(member)], tall_in)

    def load_mixer(member, slot):
        return [
            load(left_w.at[of_share(member), :], mixer_in.at[slot, 0]),
            load(right_w.at[of_share(member), :], mixer_in.at[slot, 1]),
            load(out_w.at[:, of_share(member)], mixer_in.at[slot, 2]),
        ]

    def turn(slot, scale, target):
        def step(at, carry):
            lanes = pl.ds(pl.multiple_of(at * LANES, LANES), LANES)
            target[lanes, :] = (wide_in[slot, :, lanes] * scale[lanes][None, :]).T.astype(BF16)
            return carry

        lax.fori_loop(0, wide_in.shape[2] // LANES, step, 0)

    def cast_rows(unit, stage, slot, scale):
        target = turned if stage is None else staged.at[stage]
        turn(slot, scale, target)
        member = 1 - grp if stage is None else grp
        weights[unit, :, place(fs, member)] = target[own_side, :]

    def cast_cols(unit, stage, scale):
        member = 1 - grp if stage is None else grp
        factor = scale[:, of_share(member)]
        weights[unit, :, place(fs, member)] = (tall_in[own_side, :] * factor).astype(BF16)
        if stage is not None:
            staged[stage, 0:tall, :] = (tall_in[other_side, :] * factor).astype(BF16)

    def cast_mixer(slot, member):
        at = fs * groups + member
        mixer_w[at, 0:share, :] = (mixer_in[slot, 0] * left_scale[...]).astype(BF16)
        mixer_w[at, share : 2 * share, :] = (mixer_in[slot, 1] * right_scale[...]).astype(BF16)
        mixer_w[at, 2 * share : 3 * share, :] = (
            mixer_in[slot, 2] * out_scale[:, of_share(member)]
        ).astype(BF16)

    class Piece:
        def __init__(self, slot, source):
            self.slot, self.source = slot, source

        def begin(self):
            mine = self.slot(fs, grp)
            self.first = send(self.source() if self.source else mine, mine, to_partner)
            self.second = send(mine, mine, to_near)

        def relay_first(self):
            self.first.wait_recv()
            got = self.slot(partner, grp)
            self.swaps = [send(got, got, to_group)]
            self.third = send(got, got, to_near)

        def relay_second(self):
            self.second.wait_recv()
            got = self.slot(near, grp)
            self.swaps.append(send(got, got, to_group))

        def relay_third(self):
            self.third.wait_recv()
            got = self.slot(lax.rem(near + half, count), grp)
            self.swaps.append(send(got, got, to_group))

        def complete(self):
            for copy in self.swaps:
                copy.wait_recv()

    def hidden_pieces(unit, stage, turns):
        size = tall // PIECES

        def piece(at):
            first = at * size
            away = (1 - side) * tall + first if turns else first
            return Piece(
                lambda source, member: weights.at[unit, pl.ds(first, size), place(source, member)],
                lambda: staged.at[stage, pl.ds(pl.multiple_of(away, 16), size), :],
            )

        return [piece(at) for at in range(PIECES)]

    def mixer_pieces():
        size = mixer_w.shape[1] // PIECES

        def piece(at):
            rows = pl.ds(at * size, size)
            return Piece(lambda source, member: mixer_w.at[source * groups + member, rows, :], None)

        return [piece(at) for at in range(PIECES)]

    pieces = (
        hidden_pieces(0, 0, True) + hidden_pieces(1, 1, True) + hidden_pieces(2, 2, False) + mixer_pieces()
        + hidden_pieces(3, 0, True) + hidden_pieces(4, 1, True) + hidden_pieces(5, 2, False)
    )

    begun_pieces = [2]

    def ahead(at):
        return 2 if at < 6 else 3

    def pump(at):
        pieces[at].relay_first()
        pieces[at].relay_second()
        for following in range(begun_pieces[0], min(at + ahead(at), len(pieces) - 1) + 1):
            pieces[following].begin()
            begun_pieces[0] += 1
        if at > 0:
            pieces[at - 1].relay_third()

    def complete(first, last):
        for piece in pieces[first * PIECES : last * PIECES]:
            piece.complete()


    def gather_begin(rows, pair):
        def view(at_side, at_tp, at):
            first = at_side * tokens + at * part if pair else at * part
            return rows.at[
                pl.ds(pl.multiple_of(first, part), part),
                pl.ds(pl.multiple_of(at_tp * wide, wide), wide),
            ]

        chips, cores = [], []
        for at in range(CHUNKS):
            mine = view(side, tp, at)
            chips.append(send(mine, mine, to_across))
            cores.append(send(mine, mine, to_sibling))
        return view, [], chips, cores

    def gather_pair(begun):
        view, firsts, _, _ = begun
        for at in range(CHUNKS):
            mine = view(side, tp, at)
            firsts.append(send(mine, mine, to_partner))

    def gather_end(begun):
        view, firsts, chips, cores = begun
        seconds = []
        for at in range(CHUNKS):
            if firsts:
                firsts[at].wait_recv()
                got = view(1 - side, tp, at)
                seconds.append(send(got, got, to_across))
                cores.append(send(got, got, to_sibling))
            chips[at].wait_recv()
            got = view(side, across, at)
            cores.append(send(got, got, to_sibling))
        for at, copy in enumerate(seconds):
            copy.wait_recv()
            got = view(1 - side, across, at)
            cores.append(send(got, got, to_sibling))
        for copy in cores:
            copy.wait_recv()

    def own_rows(rows, pair):
        first = pl.multiple_of(side * tokens, part) if pair else 0
        rows[pl.ds(first, tokens), pl.ds(pl.multiple_of(tp * wide, wide), wide)] = held[...]

    def norm(rows, gain):
        size = 64

        def step(at, carry):
            here = pl.ds(pl.multiple_of(at * size, size), size)
            values = rows[here, :].astype(F32)
            inverse = lax.rsqrt(jnp.mean(values * values, axis=1, keepdims=True) + EPS)
            normal[here, :] = (values * inverse * gain[...]).astype(BF16)
            return carry

        lax.fori_loop(0, rows.shape[0] // size, step, 0)

    def expand(unit):
        def step(at, carry):
            here = pl.ds(pl.multiple_of(at * tokens, tokens), tokens)
            values = normal[here, :]
            dims = (((1,), (1,)), ((), ()))
            gate = lax.dot_general(values, weights[unit], dims, preferred_element_type=F32)
            upward = lax.dot_general(values, weights[unit + 1], dims, preferred_element_type=F32)
            hidden[here, :] = (gate / (1.0 + jnp.exp(-gate)) * upward).astype(BF16)
            return carry

        lax.fori_loop(0, 2, step, 0)

    def reduce_sums(tiles, product, outs, ins, between):
        core_to, chip_to, pair_to = outs
        core_from, chip_from, pair_from = ins
        firsts, seconds, thirds = {}, {}, {}

        def begin(at):
            for to_chip in range(tps // CORES):
                other = to_chip * CORES + 1 - core
                core_to[at, to_chip] = product(tiles[at][0], other).astype(BF16)
            firsts[at] = send(core_to.at[at], core_from.at[at], to_sibling)
            for to_chip in range(tps // CORES):
                kept[at, to_chip] = product(tiles[at][0], to_chip * CORES + core)

        def chips(at):
            firsts[at].wait_recv()
            away = 1 - chip
            chip_to[at] = (kept[at, away] + core_from[at, away].astype(F32)).astype(BF16)
            seconds[at] = send(chip_to.at[at], chip_from.at[at], to_across)
            kept[at, chip] = kept[at, chip] + core_from[at, chip].astype(F32)

        def pairs(at):
            seconds[at].wait_recv()
            total = kept[at, chip] + chip_from[at].astype(F32)
            if tiles[at][1]:
                pair_to[at] = total.astype(BF16)
                thirds[at] = send(pair_to.at[at], pair_from.at[at], to_partner)
            else:
                kept[at, chip] = total

        for at in range(len(tiles) + 2):
            if at < len(tiles):
                begin(at)
            if 0 <= at - 1 < len(tiles):
                chips(at - 1)
            if 0 <= at - 2 < len(tiles):
                pairs(at - 2)
            between(at)
        own = [at for at in range(len(tiles)) if not tiles[at][1]]
        for order, at in enumerate(own):
            total = kept[at, chip]
            if thirds:
                thirds[order].wait_recv()
                total = total + pair_from[order].astype(F32)
            here = pl.ds(order * part, part)
            factor = 0.5 if thirds else 1.0
            held[here, :] = (held[here, :].astype(F32) + factor * total).astype(BF16)
        return list(firsts.values()) + list(seconds.values()) + list(thirds.values())

    def half_tiles():
        away = [((1 - side) * tokens + at * part, True) for at in range(CHUNKS)]
        return away + [(side * tokens + at * part, False) for at in range(CHUNKS)]

    def down_product(unit):
        def product(first, target):
            values = hidden[pl.ds(pl.multiple_of(first, part), part), :]
            columns = pl.ds(pl.multiple_of(target * wide, wide), wide)
            return jnp.dot(values, weights[unit, :, columns], preferred_element_type=F32)

        return product

    class Targets:
        def __init__(self, tiles, product):
            self.tiles, self.product = tiles, product
            self.order = (fs, partner, near, lax.rem(near + half, count))
            every_tile = [(step, at) for step in range(len(self.order)) for at in range(len(tiles))]
            self.cores = [
                reserve(core_out.at[at, step % 2], core_in_2.at[at, step % 2], to_sibling)
                for step, at in every_tile
            ]
            self.chips = [reserve(chip_out.at[at], chip_in_2.at[at], to_across) for _, at in every_tile]
            self.pairs = [reserve(pair_out.at[at], pair_in_2.at[at], to_partner) for at in range(CHUNKS)]

        def roles(self, step):
            target = self.order[step]
            hold = lax.rem(target, CORES) == core
            here = target // CORES == chip
            return target, hold, here

        def begin(self, step):
            target, hold, here = self.roles(step)
            size = len(self.tiles)

            def product(at):
                value = self.product(self.tiles[at][0], target)

                @pl.when(jnp.logical_not(hold))
                def _():
                    core_out[at, step % 2] = value.astype(BF16)
                    self.cores[step * size + at].start()

                @pl.when(hold)
                def _():
                    kept[at, here.astype(jnp.int32)] = value

            def add(at):
                @pl.when(hold)
                def _():
                    self.cores[step * size + at].wait_recv()
                    slot = here.astype(jnp.int32)
                    value = kept[at, slot] + core_in_2[at, step % 2].astype(F32)

                    @pl.when(here)
                    def _():
                        kept[at, 1] = value

                    @pl.when(jnp.logical_not(here))
                    def _():
                        chip_out[at] = value.astype(BF16)
                        self.chips[step * size + at].start()

            for at in range(size + 1):
                if at < size:
                    product(at)
                if at > 0:
                    add(at - 1)

        def end(self, step):
            _, hold, here = self.roles(step)
            size = len(self.tiles)

            @pl.when(jnp.logical_and(hold, here))
            def _():
                for at in range(size):
                    self.chips[step * size + at].wait_recv()
                    value = kept[at, 1] + chip_in_2[at].astype(F32)
                    if self.tiles[at][1]:
                        pair_out[at] = value.astype(BF16)
                        self.pairs[at].start()
                    else:
                        kept[at, 1] = value

        def finish(self):
            own = [at for at in range(len(self.tiles)) if not self.tiles[at][1]]
            for order, at in enumerate(own):
                self.pairs[order].wait_recv()
                total = kept[at, 1] + pair_in_2[order].astype(F32)
                here = pl.ds(order * part, part)
                held[here, :] = (held[here, :].astype(F32) + 0.5 * total).astype(BF16)

        def drain(self):
            size = len(self.tiles)
            for step in range(len(self.order)):
                _, hold, here = self.roles(step)

                @pl.when(jnp.logical_not(hold))
                def _(step=step):
                    for at in range(size):
                        self.cores[step * size + at].wait_send()

                @pl.when(jnp.logical_and(hold, jnp.logical_not(here)))
                def _(step=step):
                    for at in range(size):
                        self.chips[step * size + at].wait_send()

            for copy in self.pairs:
                copy.wait_send()


    def nothing(at):
        pass

    loads = {"g1": load_rows(gate_1, grp, 0), "u1": load_rows(up_1, grp, 1), "d1": load_cols(down_1, grp)}
    held[...] = stream[...].astype(F32).T.astype(BF16)
    own_rows(rows_1, True)
    loads["g1"].wait()
    cast_rows(0, 0, 0, gate_scale_1)
    loads["g1"] = load_rows(gate_1, 1 - grp, 0)
    pl.semaphore_wait(barrier, len(every))
    pieces[0].begin()
    pieces[1].begin()
    begun = gather_begin(rows_1, True)
    loads["u1"].wait()
    cast_rows(1, 1, 1, up_scale_1)
    loads["u1"] = load_rows(up_1, 1 - grp, 1)
    loads["d1"].wait()
    cast_cols(2, 2, down_scale_1)
    loads["d1"] = load_cols(down_1, 1 - grp)
    loads["m"] = load_mixer(grp, 0)
    loads["n"] = load_mixer(1 - grp, 1)
    loads["g1"].wait()
    cast_rows(0, None, 0, gate_scale_1)
    loads["g2"] = load_rows(gate_2, grp, 0)
    pump(0)
    loads["u1"].wait()
    cast_rows(1, None, 1, up_scale_1)
    loads["u2"] = load_rows(up_2, grp, 1)
    pump(1)
    loads["d1"].wait()
    cast_cols(2, None, down_scale_1)
    loads["d2"] = load_cols(down_2, grp)
    for copy in loads["m"] + loads["n"]:
        copy.wait()
    cast_mixer(0, grp)
    cast_mixer(1, 1 - grp)
    gather_pair(begun)
    pump(2)
    sent([piece.first for piece in pieces[0:2]])
    loads["g2"].wait()
    cast_rows(3, 0, 0, gate_scale_2)
    loads["g2"] = load_rows(gate_2, 1 - grp, 0)
    pump(3)
    gather_end(begun)
    pump(4)
    norm(rows_1, gain_1)
    sent([piece.first for piece in pieces[2:4]])
    loads["u2"].wait()
    cast_rows(4, 1, 1, up_scale_2)
    loads["u2"] = load_rows(up_2, 1 - grp, 1)
    pump(5)
    sent([piece.first for piece in pieces[4:6]])
    loads["d2"].wait()
    cast_cols(5, 2, down_scale_2)
    loads["d2"] = load_cols(down_2, 1 - grp)
    loads["g2"].wait()
    cast_rows(3, None, 0, gate_scale_2)
    loads["u2"].wait()
    cast_rows(4, None, 1, up_scale_2)
    loads["d2"].wait()
    cast_cols(5, None, down_scale_2)
    pump(6)
    complete(0, 2)
    expand(0)
    complete(2, 3)

    def between_1(at):
        if at == 3:
            pump(7)

    copies = reduce_sums(
        half_tiles(), down_product(2), (core_out, chip_out, pair_out),
        (core_in_1, chip_in_1, pair_in_1), between_1,
    )

    own_rows(rows_m, False)
    begun = gather_begin(rows_m, False)
    pump(8)
    gather_end(begun)
    norm(rows_m, gain_m)
    complete(3, 4)

    def projection(first):
        total = None
        for at in range(count * groups):
            term = jnp.dot(
                normal[0:tokens, at * share : (at + 1) * share],
                mixer_w[at, first : first + share, :],
                preferred_element_type=F32,
            )
            total = term if total is None else total + term
        return jax.nn.gelu(total)

    right = projection(share)
    lane = lax.broadcasted_iota(jnp.int32, (tokens, LANES), 1)
    summed = jnp.sum(right, axis=1, keepdims=True)
    squares = jnp.sum(right * right, axis=1, keepdims=True)
    packed = jnp.where(lane == 0, summed, jnp.where(lane == 1, squares, 0.0))
    stats[0] = packed.T[0:8, :]
    shared = [
        send(stats.at[0], stats.at[1], to_sibling),
        send(stats.at[0], stats.at[2], to_across),
        send(stats.at[0], stats.at[3], to_diagonal),
    ]
    left = projection(0)
    for copy in shared:
        copy.wait_recv()
    total = (stats[0] + stats[1]) + (stats[2] + stats[3])
    total = jnp.concatenate([total, jnp.zeros((LANES - 8, tokens), F32)], axis=0).T
    size = branch * tps
    average = total[:, 0:1] / size
    inverse = lax.rsqrt(total[:, 1:2] / size - average * average + EPS)
    centred = ((right - average) * inverse * channel_gain[...]).astype(BF16)
    span = spatial.shape[1]
    rest = jnp.zeros((span - spatial_bias.shape[0], span), F32)
    bias = jnp.concatenate([spatial_bias[...], rest], axis=0).T
    target = lax.broadcasted_iota(jnp.int32, (span, span), 0)
    source = lax.broadcasted_iota(jnp.int32, (span, span), 1)
    members = branch // spatial.shape[0]
    for group in range(spatial.shape[0]):
        matrix = jnp.where(source <= target, spatial[group].astype(F32), 0.0).astype(BF16)
        columns = slice(group * members, (group + 1) * members)
        for at in range(tokens // span):
            here = slice(at * span, (at + 1) * span)
            mixed = jnp.dot(matrix, centred[here, columns], preferred_element_type=F32)
            mixed = mixed + bias[:, group : group + 1]
            gated[here, columns] = (left[here, columns] * mixed).astype(BF16)
    pump(9)

    def out_product(first, target):
        values = gated[first : first + part, :]
        each = wide // share
        return jnp.concatenate(
            [
                jnp.dot(
                    values,
                    mixer_w[target * each + at, 2 * share : 3 * share, :],
                    preferred_element_type=F32,
                )
                for at in range(each)
            ],
            axis=1,
        )

    reduce_sums(
        [(at * part, False) for at in range(CHUNKS)], out_product, (core_out_m, chip_out_m, None),
        (core_in_m, chip_in_m, None), nothing,
    )

    own_rows(rows_2, True)
    begun = gather_begin(rows_2, True)
    gather_pair(begun)
    pump(10)
    pump(11)
    gather_end(begun)
    norm(rows_2, gain_2)
    pump(12)
    complete(4, 6)
    expand(3)
    sent(copies)
    sums = Targets(half_tiles(), down_product(5))
    last = pieces[6 * PIECES :]

    def arrived(step):
        for piece in last:
            piece.swaps[step].wait_recv()

    sums.begin(0)
    pump(13)
    arrived(0)
    sums.begin(1)
    arrived(1)
    sums.begin(2)
    last[-1].relay_third()
    sums.end(0)
    sums.end(1)
    arrived(2)
    sums.begin(3)
    sums.end(2)
    sums.end(3)
    sums.finish()
    result[...] = held[...].astype(F32).T.astype(BF16)
    for copy in list(pending):
        copy.wait_send()
    sums.drain()


def contract(left_side, right_side):
    return lax.dot_general(
        left_side, right_side, (((0,), (0,)), ((), ())), preferred_element_type=jnp.float32
    )


def product(left_side, right_side):
    return lax.dot_general(
        left_side, right_side, (((1,), (0,)), ((), ())), preferred_element_type=jnp.float32
    )


def permuted(block, axis_name, target):
    count = lax.axis_size(axis_name)
    return lax.ppermute(block, axis_name, [(at, target(at, count)) for at in range(count)])


def to_partner(block):
    return permuted(block, "fs", lambda at, count: (at + count // 2) % count)


def in_half(block, step):
    def target(at, count):
        half = count // 2
        return at // half * half + (at % half + step) % half

    return permuted(block, "fs", target)


def to_other_grp(block, step):
    return permuted(block, "grp", lambda at, count: (at + step) % count)


def to_same_core(block, step):
    return permuted(block, "tp", lambda at, count: (at + step * CORES) % count)


def to_other_core(block):
    return permuted(block, "tp", lambda at, count: at ^ 1)


def pick(blocks, index):
    count = len(blocks)
    if count == 1:
        return blocks[0]
    index = lax.rem(index + count, count)
    found = blocks[0]
    for at in range(1, count):
        found = jnp.where(index == at, blocks[at], found)
    return found


def chip_and_core():
    place = lax.axis_index("tp")
    return lax.div(place, CORES), lax.rem(place, CORES)


def gather_rows(block):
    chips = lax.axis_size("tp") // CORES
    chip, core = chip_and_core()
    held = jnp.stack([block] + [to_same_core(block, step) for step in range(1, chips)])
    other = to_other_core(held)
    found = []
    for at_chip in range(chips):
        mine = pick([held[step] for step in range(chips)], chip - at_chip)
        theirs = pick([other[step] for step in range(chips)], chip - at_chip)
        found += [jnp.where(core == 0, mine, theirs), jnp.where(core == 0, theirs, mine)]
    return jnp.concatenate(found)


def scatter_sum(terms):
    chips = lax.axis_size("tp") // CORES
    chip, core = chip_and_core()
    blocks = terms.reshape((chips, CORES, -1) + terms.shape[1:])
    mine = jnp.where(core == 0, blocks[:, 0], blocks[:, 1])
    passed = jnp.where(core == 0, blocks[:, 1], blocks[:, 0])
    pairs = mine.astype(jnp.float32) + to_other_core(passed).astype(jnp.float32)
    total = pick([pairs[at] for at in range(chips)], chip)
    for step in range(1, chips):
        sent = pick([pairs[at] for at in range(chips)], chip + step).astype(jnp.bfloat16)
        total = total + to_same_core(sent, step).astype(jnp.float32)
    return total


def places():
    count = lax.axis_size("fs")
    half = count // 2
    me = lax.axis_index("fs")
    low = lax.rem(me, half)
    found = []
    for step in range(half):
        near = me - low + lax.rem(low - step + half, half)
        found += [near, lax.rem(near + half, count)]
    return found


def shares():
    count = lax.axis_size("grp")
    me = lax.axis_index("grp")
    return [lax.rem(me - back + count, count) for back in range(count)]


def gathered(kept, passed, others):
    half = lax.axis_size("fs") // 2
    got = to_partner(passed)
    mine = [kept, got]
    for step in range(1, half):
        mine += [in_half(kept, step), in_half(got, step)]
    found = [mine]
    for back, own in zip(range(1, lax.axis_size("grp")), others):
        found.append([own] + [to_other_grp(block, back) for block in mine[1:]])
    return found


def rows_unit(weights):
    half = lax.div(lax.axis_index("fs"), lax.axis_size("fs") // 2)

    def cut(index, side):
        found = []
        for weight in weights:
            width = weight.shape[0] // lax.axis_size("grp")
            wide = weight.shape[1] // 2
            part = lax.dynamic_slice(weight, (index * width, side * wide), (width, wide))
            found.append(part.astype(jnp.bfloat16).T)
        return jnp.stack(found)

    order = shares()
    return gathered(
        cut(order[0], half), cut(order[0], 1 - half), [cut(index, half) for index in order[1:]]
    )


def cols_unit(weight):
    half = lax.div(lax.axis_index("fs"), lax.axis_size("fs") // 2)

    def cut(index, side):
        width = weight.shape[1] // lax.axis_size("grp")
        tall = weight.shape[0] // 2
        part = lax.dynamic_slice(weight, (side * tall, index * width), (tall, width))
        return part.astype(jnp.bfloat16)

    order = shares()
    return gathered(
        cut(order[0], half), cut(order[0], 1 - half), [cut(index, half) for index in order[1:]]
    )


def mixer_unit(left, right, out):
    def cut(index):
        width = left.shape[0] // lax.axis_size("grp")
        rows = [
            lax.dynamic_slice_in_dim(weight, index * width, width, 0).astype(jnp.bfloat16).T
            for weight in (left, right)
        ]
        return jnp.stack(rows + [lax.dynamic_slice_in_dim(out, index * width, width, 1).astype(jnp.bfloat16)])

    order = shares()
    share = cut(order[0])
    return gathered(share, share, [cut(index) for index in order[1:]])


def rows_in_order(rows):
    count, groups = lax.axis_size("fs"), lax.axis_size("grp")
    width = rows.shape[0] // (count * groups)
    pieces = []
    for share in shares():
        for place in places():
            pieces.append(
                lax.dynamic_slice_in_dim(rows, (place * groups + share) * width, width, 0)
            )
    return jnp.concatenate(pieces)


def joined(blocks):
    return jnp.concatenate([block for mine in blocks for block in mine], axis=-1)


def columns_out(blocks, hidden):
    count, groups = lax.axis_size("fs"), lax.axis_size("grp")
    every = joined(blocks)
    width = every.shape[1] // (count * groups)
    terms = contract(every, hidden).astype(jnp.bfloat16)
    found = jnp.zeros_like(terms)
    at = 0
    for share in shares():
        for place in places():
            found = lax.dynamic_update_slice_in_dim(
                found, terms[at : at + width], (place * groups + share) * width, 0
            )
            at += width
    return found


def inverse_of(values):
    return lax.rsqrt(jnp.mean(values * values, axis=0) + EPS)


def normed(whole_rows, gain):
    values = whole_rows.astype(jnp.float32)
    return (values * inverse_of(values) * gain[:, None]).astype(jnp.bfloat16)


def half_step(stream, gain, rows_blocks, gate_scale, up_scale, cols_blocks, down_scale):
    tokens = stream.shape[1]
    both = jnp.concatenate([stream, to_partner(stream)], axis=1)
    rows = rows_in_order(normed(gather_rows(both), gain))
    half = lax.div(lax.axis_index("fs"), lax.axis_size("fs") // 2)
    tall = gate_scale.shape[0] // 2
    gate_scale = lax.dynamic_slice_in_dim(gate_scale, half * tall, tall)[:, None]
    up_scale = lax.dynamic_slice_in_dim(up_scale, half * tall, tall)[:, None]
    every = joined(rows_blocks)
    gate = product(every[0], rows)
    upward = product(every[1], rows)
    hidden = (jax.nn.silu(gate * gate_scale) * (upward * up_scale)).astype(jnp.bfloat16)
    total = scatter_sum(columns_out(cols_blocks, hidden))
    away = to_partner(total[:, tokens:].astype(jnp.bfloat16))
    total = total[:, :tokens] + away.astype(jnp.float32)
    return (stream.astype(jnp.float32) + 0.5 * (total * down_scale[:, None])).astype(jnp.bfloat16)


def gating_unit(left_pre, right_pre, channel_gain, spatial, spatial_bias):
    left = jax.nn.gelu(left_pre)
    right = jax.nn.gelu(right_pre)
    branch = channel_gain.shape[0] * lax.axis_size("tp")
    totals, squares = lax.psum((jnp.sum(right, axis=0), jnp.sum(right * right, axis=0)), "tp")
    average = totals / branch
    inverse = lax.rsqrt(squares / branch - average * average + EPS)
    centred = ((right - average) * inverse * channel_gain[:, None]).astype(jnp.bfloat16)
    local_groups, span = (spatial.shape[0], spatial.shape[1])
    tokens = centred.shape[1]
    blocks = centred.reshape(local_groups, centred.shape[0] // local_groups, tokens // span, span)
    target = lax.broadcasted_iota(jnp.int32, (span, span), 0)
    source = lax.broadcasted_iota(jnp.int32, (span, span), 1)
    masked = jnp.where((source <= target)[None], spatial, jnp.zeros_like(spatial))
    token_mix = jnp.einsum("gts,gcns->gcnt", masked, blocks, preferred_element_type=jnp.float32)
    token_mix = token_mix + spatial_bias[:, None, None, :]
    return (left * token_mix.reshape(centred.shape[0], tokens)).astype(jnp.bfloat16)


def layer(
    stream,
    first_gain,
    first_gate,
    first_gate_scale,
    first_up,
    first_up_scale,
    first_down,
    first_down_scale,
    mixer_gain,
    mixer_left,
    mixer_left_scale,
    mixer_right,
    mixer_right_scale,
    channel_gain,
    spatial,
    spatial_bias,
    mixer_out,
    mixer_out_scale,
    second_gain,
    second_gate,
    second_gate_scale,
    second_up,
    second_up_scale,
    second_down,
    second_down_scale,
):
    held = jnp.stack([first_down_scale, mixer_out_scale, second_down_scale])
    count = lax.axis_size("fs")
    me = lax.axis_index("fs")
    parts = [held] + [
        permuted(held, "fs", lambda at, count, step=step: (at + step) % count)
        for step in range(1, count)
    ]
    scales = jnp.concatenate([pick(parts, me - place) for place in range(count)], axis=1)
    wide = stream.shape[0]
    scales = lax.dynamic_slice_in_dim(scales, lax.axis_index("tp") * wide, wide, 1)

    first_rows = rows_unit((first_gate, first_up))
    first_cols = cols_unit(first_down)
    mixer = mixer_unit(mixer_left, mixer_right, mixer_out)
    second_rows = rows_unit((second_gate, second_up))
    second_cols = cols_unit(second_down)

    stream = half_step(
        stream, first_gain, first_rows, first_gate_scale, first_up_scale, first_cols, scales[0]
    )
    rows = rows_in_order(normed(gather_rows(stream), mixer_gain))
    lefts = joined([[block[0] for block in mine] for mine in mixer])
    rights = joined([[block[1] for block in mine] for mine in mixer])
    gated = gating_unit(
        product(lefts, rows) * mixer_left_scale[:, None],
        product(rights, rows) * mixer_right_scale[:, None],
        channel_gain,
        spatial,
        spatial_bias,
    )
    total = scatter_sum(columns_out([[block[2] for block in mine] for mine in mixer], gated))
    stream = (stream.astype(jnp.float32) + total * scales[1][:, None]).astype(jnp.bfloat16)
    return half_step(
        stream, second_gain, second_rows, second_gate_scale, second_up_scale, second_cols, scales[2]
    )


def fits(stream, first_gate, mixer_left):
    groups, count, tps = lax.axis_size("grp"), lax.axis_size("fs"), lax.axis_size("tp")
    share = stream.shape[0] // groups
    tall = first_gate.shape[1] // 2
    return (
        groups == 2
        and count == 4
        and count == tps
        and tps == 2 * CORES
        and first_gate.shape[0] == stream.shape[0]
        and share % LANES == 0
        and mixer_left.shape[1] == share
        and tall % 16 == 0
        and (2 * tall) % LANES == 0
        and stream.shape[1] % (LANES * CHUNKS) == 0
        and tall % (16 * PIECES) == 0
    )


def fused(
    stream, first_gain, first_gate, first_gate_scale, first_up, first_up_scale, first_down, first_down_scale,
    mixer_gain, mixer_left, mixer_left_scale, mixer_right, mixer_right_scale, channel_gain, spatial,
    spatial_bias, mixer_out, mixer_out_scale, second_gain, second_gate, second_gate_scale, second_up,
    second_up_scale, second_down, second_down_scale,
):
    def flat(vector):
        return vector.reshape(1, -1)

    groups, count, tps = lax.axis_size("grp"), lax.axis_size("fs"), lax.axis_size("tp")
    wide, tokens = stream.shape
    share, tall, depth = wide // groups, first_gate.shape[1] // 2, wide * tps
    branch, part = mixer_left.shape[1], tokens // CHUNKS
    both = 2 * tokens
    any_spec, vmem = pl.BlockSpec(memory_space=pl.ANY), pl.BlockSpec(memory_space=pltpu.VMEM)
    chips = tps // CORES
    vm = pltpu.VMEM
    call = pl.pallas_call(
        kernel,
        out_shape=jax.ShapeDtypeStruct((wide, tokens), BF16),
        in_specs=[vmem] + [any_spec] * 9 + [vmem] * 15,
        out_specs=vmem,
        scratch_shapes=[
            vm((6, tall, depth), BF16),
            vm((count * groups, 3 * share, branch), BF16),
            vm((3, 2 * tall, share), BF16),
            vm((2 * tall, share), BF16),
            vm((2, share, 2 * tall), F32),
            vm((2 * tall, share), F32),
            vm((2, 3, share, branch), F32),
            vm((both, depth), BF16),
            vm((tokens, depth), BF16),
            vm((both, depth), BF16),
            vm((both, depth), BF16),
            vm((both, tall), BF16),
            vm((tokens, branch), BF16),
            vm((tokens, wide), BF16),
            vm((2 * CHUNKS, chips, part, wide), F32),
            vm((4, 8, tokens), F32),
            vm((2 * CHUNKS, chips, part, wide), BF16),
            vm((CHUNKS, chips, part, wide), BF16),
            vm((2 * CHUNKS, chips, part, wide), BF16),
            vm((CHUNKS, chips, part, wide), BF16),
            vm((2 * CHUNKS, chips, part, wide), BF16),
            vm((2 * CHUNKS, part, wide), BF16),
            vm((CHUNKS, part, wide), BF16),
            vm((2 * CHUNKS, part, wide), BF16),
            vm((CHUNKS, part, wide), BF16),
            vm((2 * CHUNKS, part, wide), BF16),
            vm((CHUNKS, part, wide), BF16),
            vm((CHUNKS, part, wide), BF16),
            vm((CHUNKS, part, wide), BF16),
            many(42 * PIECES + 73 * CHUNKS + 3),
            many(42 * PIECES + 73 * CHUNKS + 3),
            many(18),
        ],
        compiler_params=pltpu.CompilerParams(
            collective_id=0, has_side_effects=True, vmem_limit_bytes=67043328
        ),
    )
    return call(
        stream, first_gate, first_up, first_down, mixer_left, mixer_right, mixer_out,
        second_gate, second_up, second_down, flat(first_gain), flat(mixer_gain), flat(second_gain),
        first_gate_scale, first_up_scale, flat(first_down_scale), flat(mixer_left_scale),
        flat(mixer_right_scale), flat(mixer_out_scale), second_gate_scale, second_up_scale,
        flat(second_down_scale), flat(channel_gain), spatial, spatial_bias,
    )


def local(*args):
    if fits(args[0], args[2], args[9]):
        return fused(*args)
    return layer(*args)


def solution(mesh):
    return jax.shard_map(
        local,
        mesh=mesh,
        in_specs=(
            P("tp", ("grp", "fs")),
            P(),
            P("fs", "tp"),
            P("tp"),
            P("fs", "tp"),
            P("tp"),
            P("tp", "fs"),
            P("fs"),
            P(),
            P("fs", "tp"),
            P("tp"),
            P("fs", "tp"),
            P("tp"),
            P("tp"),
            P("tp", None, None),
            P("tp", None),
            P("tp", "fs"),
            P("fs"),
            P(),
            P("fs", "tp"),
            P("tp"),
            P("fs", "tp"),
            P("tp"),
            P("tp", "fs"),
            P("fs"),
        ),
        out_specs=P("tp", ("grp", "fs")),
        check_vma=False,
    )
```

```python
import jax
import jax.numpy as jnp
from jax import lax
from jax.experimental import pallas as pl
from jax.experimental.pallas import tpu as pltpu
from jax.sharding import PartitionSpec as P

EPS = 1e-06
CORES = 2
LANES = 128
CHUNKS = 3
PIECES = 2
SENDS = 40
AHEAD = (2, 2, 2, 2, 1, 1, 2, 2, 3)
SPLIT = 2
MESH = pl.DeviceIdType.MESH
F32, BF16 = jnp.float32, jnp.bfloat16


def many(count):
    return pltpu.SemaphoreType.DMA((count,))


def kernel(
    stream, gate_1, up_1, down_1, left_w, right_w, out_w, gate_2, up_2, down_2,
    gain_1, gain_m, gain_2, gate_scale_1, up_scale_1, down_scale_1, left_scale, right_scale, out_scale,
    gate_scale_2, up_scale_2, down_scale_2, channel_gain, spatial, spatial_bias,
    result,
    weights, mixer_w, staged, turned, wide_in, tall_in, mixer_in,
    rows_1, rows_m, rows_2, normal, hidden, gated, held, kept, stats,
    core_out, core_out_m, core_in_1, core_in_m, core_in_2,
    chip_out, chip_out_m, chip_in_1, chip_in_m, chip_in_2,
    pair_out, pair_in_1, pair_in_2,
    send_sem, recv_sem, load_sem,
):
    grp, fs, tp = lax.axis_index("grp"), lax.axis_index("fs"), lax.axis_index("tp")
    groups, count, tps = lax.axis_size("grp"), lax.axis_size("fs"), lax.axis_size("tp")
    half = count // 2
    side = fs // half
    partner = lax.rem(fs + half, count)
    near = side * half + (1 - lax.rem(fs, half))
    core, chip = lax.rem(tp, CORES), tp // CORES
    sibling = chip * CORES + (1 - core)
    across = lax.rem(tp + CORES, tps)
    diagonal = lax.rem(sibling + CORES, tps)
    wide, tokens = stream.shape
    share = wide // groups
    tall = hidden.shape[1]
    part = tokens // CHUNKS
    branch = left_w.shape[1]

    to_partner, to_near = {"fs": partner}, {"fs": near}
    to_group = {"grp": 1 - grp}
    to_sibling, to_across, to_diagonal = {"tp": sibling}, {"tp": across}, {"tp": diagonal}
    every = (to_partner, to_near, to_group, to_sibling, to_across, to_diagonal)

    barrier = pltpu.get_barrier_semaphore()
    for device in every:
        pl.semaphore_signal(barrier, inc=1, device_id=device, device_id_type=MESH)

    used = [0, 0, SENDS]
    pending, taken, slots = [], [], list(range(SENDS))

    def send(source, target, device):
        if not slots:
            sent([pending[0]])
        slot = slots.pop(0)
        at = used[0]
        used[0] += 1
        copy = pltpu.make_async_remote_copy(
            src_ref=source,
            dst_ref=target,
            send_sem=send_sem.at[slot],
            recv_sem=recv_sem.at[at],
            device_id=device,
            device_id_type=MESH,
        )
        copy.start()
        pending.append(copy)
        taken.append(slot)
        return copy

    def reserve(source, target, device):
        at = used[0]
        used[0] += 1
        used[2] += 1
        return pltpu.make_async_remote_copy(
            src_ref=source,
            dst_ref=target,
            send_sem=send_sem.at[used[2] - 1],
            recv_sem=recv_sem.at[at],
            device_id=device,
            device_id_type=MESH,
        )

    def sent(copies):
        for copy in copies:
            for at, other in enumerate(pending):
                if other is copy:
                    copy.wait_send()
                    pending.pop(at)
                    slots.append(taken.pop(at))
                    break

    def load(source, target):
        at = used[1]
        used[1] += 1
        copy = pltpu.make_async_copy(source, target, load_sem.at[at])
        copy.start()
        return copy

    def place(source, member):
        return pl.ds(pl.multiple_of((source * groups + member) * share, share), share)

    def of_share(member):
        return pl.ds(pl.multiple_of(member * share, share), share)

    own_side = pl.ds(pl.multiple_of(side * tall, 16), tall)
    other_side = pl.ds(pl.multiple_of((1 - side) * tall, 16), tall)


    def load_rows(weight, member, slot):
        return load(weight.at[of_share(member), :], wide_in.at[slot])

    def load_cols(weight, member):
        return load(weight.at[:, of_share(member)], tall_in)

    def load_mixer(member, slot):
        return [
            load(left_w.at[of_share(member), :], mixer_in.at[slot, 0]),
            load(right_w.at[of_share(member), :], mixer_in.at[slot, 1]),
            load(out_w.at[:, of_share(member)], mixer_in.at[slot, 2]),
        ]

    def turn(slot, scale, target):
        def step(at, carry):
            lanes = pl.ds(pl.multiple_of(at * LANES, LANES), LANES)
            target[lanes, :] = (wide_in[slot, :, lanes] * scale[lanes][None, :]).T.astype(BF16)
            return carry

        lax.fori_loop(0, wide_in.shape[2] // LANES, step, 0)

    def cast_rows(unit, stage, slot, scale):
        target = turned if stage is None else staged.at[stage]
        turn(slot, scale, target)
        member = 1 - grp if stage is None else grp
        weights[unit, :, place(fs, member)] = target[own_side, :]

    def cast_cols(unit, stage, scale):
        member = 1 - grp if stage is None else grp
        factor = scale[:, of_share(member)]
        weights[unit, :, place(fs, member)] = (tall_in[own_side, :] * factor).astype(BF16)
        if stage is not None:
            staged[stage, 0:tall, :] = (tall_in[other_side, :] * factor).astype(BF16)

    def cast_mixer(slot, member):
        at = fs * groups + member
        mixer_w[at, 0:share, :] = (mixer_in[slot, 0] * left_scale[...]).astype(BF16)
        mixer_w[at, share : 2 * share, :] = (mixer_in[slot, 1] * right_scale[...]).astype(BF16)
        mixer_w[at, 2 * share : 3 * share, :] = (
            mixer_in[slot, 2] * out_scale[:, of_share(member)]
        ).astype(BF16)

    class Piece:
        def __init__(self, slot, source):
            self.slot, self.source = slot, source

        def begin(self):
            mine = self.slot(fs, grp)
            self.first = send(self.source() if self.source else mine, mine, to_partner)
            self.second = send(mine, mine, to_near)

        def relay_first(self):
            self.first.wait_recv()
            got = self.slot(partner, grp)
            self.swaps = [send(got, got, to_group)]
            self.third = send(got, got, to_near)

        def relay_second(self):
            self.second.wait_recv()
            got = self.slot(near, grp)
            self.swaps.append(send(got, got, to_group))

        def relay_third(self):
            self.third.wait_recv()
            got = self.slot(lax.rem(near + half, count), grp)
            self.swaps.append(send(got, got, to_group))

        def complete(self):
            for copy in self.swaps:
                copy.wait_recv()

    def hidden_pieces(unit, stage, turns):
        size = tall // PIECES

        def piece(at):
            first = at * size
            away = (1 - side) * tall + first if turns else first
            return Piece(
                lambda source, member: weights.at[unit, pl.ds(first, size), place(source, member)],
                lambda: staged.at[stage, pl.ds(pl.multiple_of(away, 16), size), :],
            )

        return [piece(at) for at in range(PIECES)]

    def mixer_pieces():
        size = mixer_w.shape[1] // PIECES

        def piece(at):
            rows = pl.ds(at * size, size)
            return Piece(lambda source, member: mixer_w.at[source * groups + member, rows, :], None)

        return [piece(at) for at in range(PIECES)]

    pieces = (
        hidden_pieces(0, 0, True) + hidden_pieces(1, 1, True) + hidden_pieces(2, 2, False) + mixer_pieces()
        + hidden_pieces(3, 0, True) + hidden_pieces(4, 1, True) + hidden_pieces(5, 2, False)
    )

    begun_pieces = [2]

    def ahead(at):
        return AHEAD[min(at, len(AHEAD) - 1)]

    def pump(at):
        pieces[at].relay_first()
        pieces[at].relay_second()
        for following in range(begun_pieces[0], min(at + ahead(at), len(pieces) - 1) + 1):
            pieces[following].begin()
            begun_pieces[0] += 1

    def third(at):
        pieces[at].relay_third()

    def complete(first, last):
        for piece in pieces[first * PIECES : last * PIECES]:
            piece.complete()


    def gather_begin(rows, pair):
        def view(at_side, at_tp, at):
            first = at_side * tokens + at * part if pair else at * part
            return rows.at[
                pl.ds(pl.multiple_of(first, part), part),
                pl.ds(pl.multiple_of(at_tp * wide, wide), wide),
            ]

        chips, cores = [], []
        for at in range(CHUNKS):
            mine = view(side, tp, at)
            chips.append(send(mine, mine, to_across))
            cores.append(send(mine, mine, to_sibling))
        return view, [], chips, cores

    def gather_pair(begun):
        view, firsts, _, _ = begun
        size = wide // SPLIT
        for at in range(CHUNKS):
            mine = view(side, tp, at)
            narrow = [mine.at[:, first * size : (first + 1) * size] for first in range(SPLIT)]
            firsts.append([send(block, block, to_partner) for block in narrow])

    def relay_own(begun):
        view, _, chips, cores = begun
        for at in range(CHUNKS):
            chips[at].wait_recv()
            got = view(side, across, at)
            cores.append(send(got, got, to_sibling))

    def relay_pair(begun):
        view, firsts, _, _ = begun
        seconds, cores = [], []
        for at in range(CHUNKS):
            for copy in firsts[at]:
                copy.wait_recv()
            got = view(1 - side, tp, at)
            seconds.append(send(got, got, to_across))
            cores.append(send(got, got, to_sibling))
        return seconds, cores

    def end_own(begun):
        for copy in begun[3]:
            copy.wait_recv()

    def end_pair(begun, relayed):
        view = begun[0]
        seconds, cores = relayed
        for at, copy in enumerate(seconds):
            copy.wait_recv()
            got = view(1 - side, across, at)
            cores.append(send(got, got, to_sibling))
        for copy in cores:
            copy.wait_recv()

    def own_rows(rows, pair):
        first = pl.multiple_of(side * tokens, part) if pair else 0
        rows[pl.ds(first, tokens), pl.ds(pl.multiple_of(tp * wide, wide), wide)] = held[...]

    def norm(rows, gain, first):
        size = 64

        def step(at, carry):
            here = pl.ds(pl.multiple_of(first + at * size, size), size)
            values = rows[here, :].astype(F32)
            inverse = lax.rsqrt(jnp.mean(values * values, axis=1, keepdims=True) + EPS)
            normal[here, :] = (values * inverse * gain[...]).astype(BF16)
            return carry

        lax.fori_loop(0, tokens // size, step, 0)

    def expand(unit):
        def step(at, carry):
            here = pl.ds(pl.multiple_of(at * tokens, tokens), tokens)
            values = normal[here, :]
            dims = (((1,), (1,)), ((), ()))
            gate = lax.dot_general(values, weights[unit], dims, preferred_element_type=F32)
            upward = lax.dot_general(values, weights[unit + 1], dims, preferred_element_type=F32)
            hidden[here, :] = (gate / (1.0 + jnp.exp(-gate)) * upward).astype(BF16)
            return carry

        lax.fori_loop(0, 2, step, 0)

    def reduce_sums(tiles, product, outs, ins, between):
        core_to, chip_to, pair_to = outs
        core_from, chip_from, pair_from = ins
        firsts, seconds, thirds = {}, {}, {}
        size = wide // SPLIT
        halves = [slice(at * size, (at + 1) * size) for at in range(SPLIT)]

        def begin(at):
            for to_chip in range(tps // CORES):
                other = to_chip * CORES + 1 - core
                core_to[at, to_chip] = product(tiles[at][0], other).astype(BF16)
            firsts[at] = send(core_to.at[at], core_from.at[at], to_sibling)
            for to_chip in range(tps // CORES):
                kept[at, to_chip] = product(tiles[at][0], to_chip * CORES + core)

        def chips(at):
            firsts[at].wait_recv()
            away = 1 - chip
            chip_to[at] = (kept[at, away] + core_from[at, away].astype(F32)).astype(BF16)
            seconds[at] = send(chip_to.at[at], chip_from.at[at], to_across)
            kept[at, chip] = kept[at, chip] + core_from[at, chip].astype(F32)

        def pairs(at):
            seconds[at].wait_recv()
            total = kept[at, chip] + chip_from[at].astype(F32)
            if tiles[at][1]:
                pair_to[at] = total.astype(BF16)
                thirds[at] = [
                    send(pair_to.at[at, :, columns], pair_from.at[at, :, columns], to_partner)
                    for columns in halves
                ]
            else:
                kept[at, chip] = total

        for at in range(len(tiles) + 2):
            if at < len(tiles):
                begin(at)
            if 0 <= at - 1 < len(tiles):
                chips(at - 1)
            if 0 <= at - 2 < len(tiles):
                pairs(at - 2)
            between(at)
        own = [at for at in range(len(tiles)) if not tiles[at][1]]
        for order, at in enumerate(own):
            total = kept[at, chip]
            if thirds:
                for copy in thirds[order]:
                    copy.wait_recv()
                total = total + pair_from[order].astype(F32)
            here = pl.ds(order * part, part)
            factor = 0.5 if thirds else 1.0
            held[here, :] = (held[here, :].astype(F32) + factor * total).astype(BF16)
        return list(firsts.values()) + list(seconds.values()) + sum(thirds.values(), [])

    def half_tiles():
        away = [((1 - side) * tokens + at * part, True) for at in range(CHUNKS)]
        return away + [(side * tokens + at * part, False) for at in range(CHUNKS)]

    def down_product(unit):
        def product(first, target):
            values = hidden[pl.ds(pl.multiple_of(first, part), part), :]
            columns = pl.ds(pl.multiple_of(target * wide, wide), wide)
            return jnp.dot(values, weights[unit, :, columns], preferred_element_type=F32)

        return product

    class Targets:
        def __init__(self, tiles, product):
            self.tiles, self.product = tiles, product
            self.order = (fs, partner, near, lax.rem(near + half, count))
            self.cores = [
                reserve(core_out.at[at, step], core_in_2.at[at, step], to_sibling)
                for step in range(2)
                for at in range(len(tiles))
            ]
            self.chips = [reserve(chip_out.at[at], chip_in_2.at[at], to_across) for at in range(len(tiles))]
            self.pairs = [reserve(pair_out.at[at], pair_in_2.at[at], to_partner) for at in range(CHUNKS)]

        def roles(self, step):
            target = self.order[step]
            hold = lax.rem(target, CORES) == core
            here = target // CORES == chip
            return target, hold, here

        def begin(self, step, pair):
            target, hold, here = self.roles(step)
            size = len(self.tiles)
            chosen = [at for at in range(size) if self.tiles[at][1] == pair]

            def product(at):
                value = self.product(self.tiles[at][0], target)

                @pl.when(jnp.logical_not(hold))
                def _():
                    core_out[at, step % 2] = value.astype(BF16)
                    self.cores[step % 2 * size + at].start()

                @pl.when(hold)
                def _():
                    kept[at, here.astype(jnp.int32)] = value

            def add(at):
                @pl.when(hold)
                def _():
                    self.cores[step % 2 * size + at].wait_recv()
                    slot = here.astype(jnp.int32)
                    value = kept[at, slot] + core_in_2[at, step % 2].astype(F32)

                    @pl.when(here)
                    def _():
                        kept[at, 1] = value

                    @pl.when(jnp.logical_not(here))
                    def _():
                        chip_out[at] = value.astype(BF16)
                        self.chips[at].start()

            for order in range(len(chosen) + 1):
                if order < len(chosen):
                    product(chosen[order])
                if order > 0:
                    add(chosen[order - 1])

        def end(self, step, pair):
            _, hold, here = self.roles(step)
            chosen = [at for at in range(len(self.tiles)) if self.tiles[at][1] == pair]

            @pl.when(jnp.logical_and(hold, here))
            def _():
                for at in chosen:
                    self.chips[at].wait_recv()
                    value = kept[at, 1] + chip_in_2[at].astype(F32)
                    if self.tiles[at][1]:
                        pair_out[at] = value.astype(BF16)
                        self.pairs[at].start()
                    else:
                        kept[at, 1] = value

        def finish(self):
            own = [at for at in range(len(self.tiles)) if not self.tiles[at][1]]
            for order, at in enumerate(own):
                self.pairs[order].wait_recv()
                total = kept[at, 1] + pair_in_2[order].astype(F32)
                here = pl.ds(order * part, part)
                held[here, :] = (held[here, :].astype(F32) + 0.5 * total).astype(BF16)

        def drain(self):
            size = len(self.tiles)
            for step in range(len(self.order)):
                _, hold, here = self.roles(step)

                @pl.when(jnp.logical_not(hold))
                def _(step=step):
                    for at in range(size):
                        self.cores[step % 2 * size + at].wait_send()

                @pl.when(jnp.logical_and(hold, jnp.logical_not(here)))
                def _(step=step):
                    for at in range(size):
                        self.chips[at].wait_send()

            for copy in self.pairs:
                copy.wait_send()


    loads = {"g1": load_rows(gate_1, grp, 0), "u1": load_rows(up_1, grp, 1), "d1": load_cols(down_1, grp)}
    held[...] = stream[...].astype(F32).T.astype(BF16)
    own_rows(rows_1, True)
    loads["g1"].wait()
    cast_rows(0, 0, 0, gate_scale_1)
    loads["g1"] = load_rows(gate_1, 1 - grp, 0)
    pl.semaphore_wait(barrier, len(every))
    pieces[0].begin()
    pieces[1].begin()
    begun = gather_begin(rows_1, True)
    loads["u1"].wait()
    cast_rows(1, 1, 1, up_scale_1)
    loads["u1"] = load_rows(up_1, 1 - grp, 1)
    loads["d1"].wait()
    cast_cols(2, 2, down_scale_1)
    loads["d1"] = load_cols(down_1, 1 - grp)
    loads["m"] = load_mixer(grp, 0)
    loads["n"] = load_mixer(1 - grp, 1)
    loads["g1"].wait()
    cast_rows(0, None, 0, gate_scale_1)
    loads["g2"] = load_rows(gate_2, grp, 0)
    pump(0)
    loads["u1"].wait()
    cast_rows(1, None, 1, up_scale_1)
    loads["u2"] = load_rows(up_2, grp, 1)
    pump(1)
    loads["d1"].wait()
    cast_cols(2, None, down_scale_1)
    loads["d2"] = load_cols(down_2, grp)
    for copy in loads["m"] + loads["n"]:
        copy.wait()
    cast_mixer(0, grp)
    cast_mixer(1, 1 - grp)
    third(0)
    gather_pair(begun)
    pump(2)
    sent([piece.first for piece in pieces[0:2]])
    loads["g2"].wait()
    cast_rows(3, 0, 0, gate_scale_2)
    loads["g2"] = load_rows(gate_2, 1 - grp, 0)
    third(1)
    pump(3)
    relay_own(begun)
    relayed = relay_pair(begun)
    third(2)
    sent([piece.first for piece in pieces[2:4]])
    loads["u2"].wait()
    cast_rows(4, 1, 1, up_scale_2)
    loads["u2"] = load_rows(up_2, 1 - grp, 1)
    pump(4)
    end_own(begun)
    end_pair(begun, relayed)
    norm(rows_1, gain_1, 0)
    norm(rows_1, gain_1, tokens)
    third(3)
    loads["g2"].wait()
    cast_rows(3, None, 0, gate_scale_2)
    pump(5)
    sent([piece.first for piece in pieces[4:6]])
    loads["d2"].wait()
    cast_cols(5, 2, down_scale_2)
    loads["d2"] = load_cols(down_2, 1 - grp)
    third(4)
    loads["u2"].wait()
    cast_rows(4, None, 1, up_scale_2)
    loads["d2"].wait()
    cast_cols(5, None, down_scale_2)
    pump(6)
    third(5)
    complete(0, 2)
    expand(0)
    complete(2, 3)

    def between_1(at):
        if at == 0:
            pump(7)
        if at == 3:
            third(6)
        if at == 5:
            pump(8)
        if at == 7:
            third(7)

    copies = reduce_sums(
        half_tiles(), down_product(2), (core_out, chip_out, pair_out),
        (core_in_1, chip_in_1, pair_in_1), between_1,
    )

    own_rows(rows_m, False)
    begun = gather_begin(rows_m, False)
    pump(9)
    relay_own(begun)
    end_own(begun)
    norm(rows_m, gain_m, 0)
    third(8)
    complete(3, 4)

    def projection(first):
        total = None
        for at in range(count * groups):
            term = jnp.dot(
                normal[0:tokens, at * share : (at + 1) * share],
                mixer_w[at, first : first + share, :],
                preferred_element_type=F32,
            )
            total = term if total is None else total + term
        return jax.nn.gelu(total)

    right = projection(share)
    lane = lax.broadcasted_iota(jnp.int32, (tokens, LANES), 1)
    summed = jnp.sum(right, axis=1, keepdims=True)
    squares = jnp.sum(right * right, axis=1, keepdims=True)
    packed = jnp.where(lane == 0, summed, jnp.where(lane == 1, squares, 0.0))
    stats[0] = packed.T[0:8, :]
    shared = [
        send(stats.at[0], stats.at[1], to_sibling),
        send(stats.at[0], stats.at[2], to_across),
        send(stats.at[0], stats.at[3], to_diagonal),
    ]
    left = projection(0)
    pump(10)
    for copy in shared:
        copy.wait_recv()
    total = (stats[0] + stats[1]) + (stats[2] + stats[3])
    total = jnp.concatenate([total, jnp.zeros((LANES - 8, tokens), F32)], axis=0).T
    size = branch * tps
    average = total[:, 0:1] / size
    inverse = lax.rsqrt(total[:, 1:2] / size - average * average + EPS)
    centred = ((right - average) * inverse * channel_gain[...]).astype(BF16)
    span = spatial.shape[1]
    rest = jnp.zeros((span - spatial_bias.shape[0], span), F32)
    bias = jnp.concatenate([spatial_bias[...], rest], axis=0).T
    target = lax.broadcasted_iota(jnp.int32, (span, span), 0)
    source = lax.broadcasted_iota(jnp.int32, (span, span), 1)
    members = branch // spatial.shape[0]
    for group in range(spatial.shape[0]):
        matrix = jnp.where(source <= target, spatial[group].astype(F32), 0.0).astype(BF16)
        columns = slice(group * members, (group + 1) * members)
        for at in range(tokens // span):
            here = slice(at * span, (at + 1) * span)
            mixed = jnp.dot(matrix, centred[here, columns], preferred_element_type=F32)
            mixed = mixed + bias[:, group : group + 1]
            gated[here, columns] = (left[here, columns] * mixed).astype(BF16)

    def out_product(first, target):
        values = gated[first : first + part, :]
        each = wide // share
        return jnp.concatenate(
            [
                jnp.dot(
                    values,
                    mixer_w[target * each + at, 2 * share : 3 * share, :],
                    preferred_element_type=F32,
                )
                for at in range(each)
            ],
            axis=1,
        )

    def between_m(at):
        if at == 2:
            third(9)
        if at == 4:
            pump(11)

    reduce_sums(
        [(at * part, False) for at in range(CHUNKS)], out_product, (core_out_m, chip_out_m, None),
        (core_in_m, chip_in_m, None), between_m,
    )

    own_rows(rows_2, True)
    begun = gather_begin(rows_2, True)
    gather_pair(begun)
    third(10)
    relay_own(begun)
    pump(12)
    third(11)
    relayed = relay_pair(begun)
    end_own(begun)
    norm(rows_2, gain_2, side * tokens)
    pump(13)
    end_pair(begun, relayed)
    norm(rows_2, gain_2, (1 - side) * tokens)
    third(12)
    complete(4, 6)
    expand(3)
    sent(copies)
    sums = Targets(half_tiles(), down_product(5))
    last = pieces[6 * PIECES :]

    def arrived(step):
        for piece in last:
            piece.swaps[step].wait_recv()

    third(13)
    sums.begin(0, True)
    arrived(0)
    sums.begin(1, True)
    arrived(1)
    sums.begin(2, True)
    sums.end(0, True)
    sums.end(1, True)
    arrived(2)
    sums.begin(3, True)
    sums.begin(0, False)
    sums.begin(1, False)
    sums.end(2, True)
    sums.end(3, True)
    sums.begin(2, False)
    sums.begin(3, False)
    for step in range(count):
        sums.end(step, False)
    sums.finish()
    result[...] = held[...].astype(F32).T.astype(BF16)
    sent(list(pending))
    sums.drain()


def contract(left_side, right_side):
    return lax.dot_general(
        left_side, right_side, (((0,), (0,)), ((), ())), preferred_element_type=jnp.float32
    )


def product(left_side, right_side):
    return lax.dot_general(
        left_side, right_side, (((1,), (0,)), ((), ())), preferred_element_type=jnp.float32
    )


def permuted(block, axis_name, target):
    count = lax.axis_size(axis_name)
    return lax.ppermute(block, axis_name, [(at, target(at, count)) for at in range(count)])


def to_partner(block):
    return permuted(block, "fs", lambda at, count: (at + count // 2) % count)


def in_half(block, step):
    def target(at, count):
        half = count // 2
        return at // half * half + (at % half + step) % half

    return permuted(block, "fs", target)


def to_other_grp(block, step):
    return permuted(block, "grp", lambda at, count: (at + step) % count)


def to_same_core(block, step):
    return permuted(block, "tp", lambda at, count: (at + step * CORES) % count)


def to_other_core(block):
    return permuted(block, "tp", lambda at, count: at ^ 1)


def pick(blocks, index):
    count = len(blocks)
    if count == 1:
        return blocks[0]
    index = lax.rem(index + count, count)
    found = blocks[0]
    for at in range(1, count):
        found = jnp.where(index == at, blocks[at], found)
    return found


def chip_and_core():
    place = lax.axis_index("tp")
    return lax.div(place, CORES), lax.rem(place, CORES)


def gather_rows(block):
    chips = lax.axis_size("tp") // CORES
    chip, core = chip_and_core()
    held = jnp.stack([block] + [to_same_core(block, step) for step in range(1, chips)])
    other = to_other_core(held)
    found = []
    for at_chip in range(chips):
        mine = pick([held[step] for step in range(chips)], chip - at_chip)
        theirs = pick([other[step] for step in range(chips)], chip - at_chip)
        found += [jnp.where(core == 0, mine, theirs), jnp.where(core == 0, theirs, mine)]
    return jnp.concatenate(found)


def scatter_sum(terms):
    chips = lax.axis_size("tp") // CORES
    chip, core = chip_and_core()
    blocks = terms.reshape((chips, CORES, -1) + terms.shape[1:])
    mine = jnp.where(core == 0, blocks[:, 0], blocks[:, 1])
    passed = jnp.where(core == 0, blocks[:, 1], blocks[:, 0])
    pairs = mine.astype(jnp.float32) + to_other_core(passed).astype(jnp.float32)
    total = pick([pairs[at] for at in range(chips)], chip)
    for step in range(1, chips):
        sent = pick([pairs[at] for at in range(chips)], chip + step).astype(jnp.bfloat16)
        total = total + to_same_core(sent, step).astype(jnp.float32)
    return total


def places():
    count = lax.axis_size("fs")
    half = count // 2
    me = lax.axis_index("fs")
    low = lax.rem(me, half)
    found = []
    for step in range(half):
        near = me - low + lax.rem(low - step + half, half)
        found += [near, lax.rem(near + half, count)]
    return found


def shares():
    count = lax.axis_size("grp")
    me = lax.axis_index("grp")
    return [lax.rem(me - back + count, count) for back in range(count)]


def gathered(kept, passed, others):
    half = lax.axis_size("fs") // 2
    got = to_partner(passed)
    mine = [kept, got]
    for step in range(1, half):
        mine += [in_half(kept, step), in_half(got, step)]
    found = [mine]
    for back, own in zip(range(1, lax.axis_size("grp")), others):
        found.append([own] + [to_other_grp(block, back) for block in mine[1:]])
    return found


def rows_unit(weights):
    half = lax.div(lax.axis_index("fs"), lax.axis_size("fs") // 2)

    def cut(index, side):
        found = []
        for weight in weights:
            width = weight.shape[0] // lax.axis_size("grp")
            wide = weight.shape[1] // 2
            part = lax.dynamic_slice(weight, (index * width, side * wide), (width, wide))
            found.append(part.astype(jnp.bfloat16).T)
        return jnp.stack(found)

    order = shares()
    return gathered(
        cut(order[0], half), cut(order[0], 1 - half), [cut(index, half) for index in order[1:]]
    )


def cols_unit(weight):
    half = lax.div(lax.axis_index("fs"), lax.axis_size("fs") // 2)

    def cut(index, side):
        width = weight.shape[1] // lax.axis_size("grp")
        tall = weight.shape[0] // 2
        part = lax.dynamic_slice(weight, (side * tall, index * width), (tall, width))
        return part.astype(jnp.bfloat16)

    order = shares()
    return gathered(
        cut(order[0], half), cut(order[0], 1 - half), [cut(index, half) for index in order[1:]]
    )


def mixer_unit(left, right, out):
    def cut(index):
        width = left.shape[0] // lax.axis_size("grp")
        rows = [
            lax.dynamic_slice_in_dim(weight, index * width, width, 0).astype(jnp.bfloat16).T
            for weight in (left, right)
        ]
        return jnp.stack(rows + [lax.dynamic_slice_in_dim(out, index * width, width, 1).astype(jnp.bfloat16)])

    order = shares()
    share = cut(order[0])
    return gathered(share, share, [cut(index) for index in order[1:]])


def rows_in_order(rows):
    count, groups = lax.axis_size("fs"), lax.axis_size("grp")
    width = rows.shape[0] // (count * groups)
    pieces = []
    for share in shares():
        for place in places():
            pieces.append(
                lax.dynamic_slice_in_dim(rows, (place * groups + share) * width, width, 0)
            )
    return jnp.concatenate(pieces)


def joined(blocks):
    return jnp.concatenate([block for mine in blocks for block in mine], axis=-1)


def columns_out(blocks, hidden):
    count, groups = lax.axis_size("fs"), lax.axis_size("grp")
    every = joined(blocks)
    width = every.shape[1] // (count * groups)
    terms = contract(every, hidden).astype(jnp.bfloat16)
    found = jnp.zeros_like(terms)
    at = 0
    for share in shares():
        for place in places():
            found = lax.dynamic_update_slice_in_dim(
                found, terms[at : at + width], (place * groups + share) * width, 0
            )
            at += width
    return found


def inverse_of(values):
    return lax.rsqrt(jnp.mean(values * values, axis=0) + EPS)


def normed(whole_rows, gain):
    values = whole_rows.astype(jnp.float32)
    return (values * inverse_of(values) * gain[:, None]).astype(jnp.bfloat16)


def half_step(stream, gain, rows_blocks, gate_scale, up_scale, cols_blocks, down_scale):
    tokens = stream.shape[1]
    both = jnp.concatenate([stream, to_partner(stream)], axis=1)
    rows = rows_in_order(normed(gather_rows(both), gain))
    half = lax.div(lax.axis_index("fs"), lax.axis_size("fs") // 2)
    tall = gate_scale.shape[0] // 2
    gate_scale = lax.dynamic_slice_in_dim(gate_scale, half * tall, tall)[:, None]
    up_scale = lax.dynamic_slice_in_dim(up_scale, half * tall, tall)[:, None]
    every = joined(rows_blocks)
    gate = product(every[0], rows)
    upward = product(every[1], rows)
    hidden = (jax.nn.silu(gate * gate_scale) * (upward * up_scale)).astype(jnp.bfloat16)
    total = scatter_sum(columns_out(cols_blocks, hidden))
    away = to_partner(total[:, tokens:].astype(jnp.bfloat16))
    total = total[:, :tokens] + away.astype(jnp.float32)
    return (stream.astype(jnp.float32) + 0.5 * (total * down_scale[:, None])).astype(jnp.bfloat16)


def gating_unit(left_pre, right_pre, channel_gain, spatial, spatial_bias):
    left = jax.nn.gelu(left_pre)
    right = jax.nn.gelu(right_pre)
    branch = channel_gain.shape[0] * lax.axis_size("tp")
    totals, squares = lax.psum((jnp.sum(right, axis=0), jnp.sum(right * right, axis=0)), "tp")
    average = totals / branch
    inverse = lax.rsqrt(squares / branch - average * average + EPS)
    centred = ((right - average) * inverse * channel_gain[:, None]).astype(jnp.bfloat16)
    local_groups, span = (spatial.shape[0], spatial.shape[1])
    tokens = centred.shape[1]
    blocks = centred.reshape(local_groups, centred.shape[0] // local_groups, tokens // span, span)
    target = lax.broadcasted_iota(jnp.int32, (span, span), 0)
    source = lax.broadcasted_iota(jnp.int32, (span, span), 1)
    masked = jnp.where((source <= target)[None], spatial, jnp.zeros_like(spatial))
    token_mix = jnp.einsum("gts,gcns->gcnt", masked, blocks, preferred_element_type=jnp.float32)
    token_mix = token_mix + spatial_bias[:, None, None, :]
    return (left * token_mix.reshape(centred.shape[0], tokens)).astype(jnp.bfloat16)


def layer(
    stream,
    first_gain,
    first_gate,
    first_gate_scale,
    first_up,
    first_up_scale,
    first_down,
    first_down_scale,
    mixer_gain,
    mixer_left,
    mixer_left_scale,
    mixer_right,
    mixer_right_scale,
    channel_gain,
    spatial,
    spatial_bias,
    mixer_out,
    mixer_out_scale,
    second_gain,
    second_gate,
    second_gate_scale,
    second_up,
    second_up_scale,
    second_down,
    second_down_scale,
):
    held = jnp.stack([first_down_scale, mixer_out_scale, second_down_scale])
    count = lax.axis_size("fs")
    me = lax.axis_index("fs")
    parts = [held] + [
        permuted(held, "fs", lambda at, count, step=step: (at + step) % count)
        for step in range(1, count)
    ]
    scales = jnp.concatenate([pick(parts, me - place) for place in range(count)], axis=1)
    wide = stream.shape[0]
    scales = lax.dynamic_slice_in_dim(scales, lax.axis_index("tp") * wide, wide, 1)

    first_rows = rows_unit((first_gate, first_up))
    first_cols = cols_unit(first_down)
    mixer = mixer_unit(mixer_left, mixer_right, mixer_out)
    second_rows = rows_unit((second_gate, second_up))
    second_cols = cols_unit(second_down)

    stream = half_step(
        stream, first_gain, first_rows, first_gate_scale, first_up_scale, first_cols, scales[0]
    )
    rows = rows_in_order(normed(gather_rows(stream), mixer_gain))
    lefts = joined([[block[0] for block in mine] for mine in mixer])
    rights = joined([[block[1] for block in mine] for mine in mixer])
    gated = gating_unit(
        product(lefts, rows) * mixer_left_scale[:, None],
        product(rights, rows) * mixer_right_scale[:, None],
        channel_gain,
        spatial,
        spatial_bias,
    )
    total = scatter_sum(columns_out([[block[2] for block in mine] for mine in mixer], gated))
    stream = (stream.astype(jnp.float32) + total * scales[1][:, None]).astype(jnp.bfloat16)
    return half_step(
        stream, second_gain, second_rows, second_gate_scale, second_up_scale, second_cols, scales[2]
    )


def fits(stream, first_gate, mixer_left):
    groups, count, tps = lax.axis_size("grp"), lax.axis_size("fs"), lax.axis_size("tp")
    share = stream.shape[0] // groups
    tall = first_gate.shape[1] // 2
    return (
        groups == 2
        and count == 4
        and count == tps
        and tps == 2 * CORES
        and first_gate.shape[0] == stream.shape[0]
        and share % LANES == 0
        and mixer_left.shape[1] == share
        and tall % 16 == 0
        and (2 * tall) % LANES == 0
        and stream.shape[0] % (LANES * SPLIT) == 0
        and stream.shape[1] % (LANES * CHUNKS) == 0
        and tall % (16 * PIECES) == 0
    )


def fused(
    stream, first_gain, first_gate, first_gate_scale, first_up, first_up_scale, first_down, first_down_scale,
    mixer_gain, mixer_left, mixer_left_scale, mixer_right, mixer_right_scale, channel_gain, spatial,
    spatial_bias, mixer_out, mixer_out_scale, second_gain, second_gate, second_gate_scale, second_up,
    second_up_scale, second_down, second_down_scale,
):
    def flat(vector):
        return vector.reshape(1, -1)

    groups, count, tps = lax.axis_size("grp"), lax.axis_size("fs"), lax.axis_size("tp")
    wide, tokens = stream.shape
    share, tall, depth = wide // groups, first_gate.shape[1] // 2, wide * tps
    branch, part = mixer_left.shape[1], tokens // CHUNKS
    both = 2 * tokens
    any_spec, vmem = pl.BlockSpec(memory_space=pl.ANY), pl.BlockSpec(memory_space=pltpu.VMEM)
    chips = tps // CORES
    vm = pltpu.VMEM
    call = pl.pallas_call(
        kernel,
        out_shape=jax.ShapeDtypeStruct((wide, tokens), BF16),
        in_specs=[vmem] + [any_spec] * 9 + [vmem] * 15,
        out_specs=vmem,
        scratch_shapes=[
            vm((6, tall, depth), BF16),
            vm((count * groups, 3 * share, branch), BF16),
            vm((3, 2 * tall, share), BF16),
            vm((2 * tall, share), BF16),
            vm((2, share, 2 * tall), F32),
            vm((2 * tall, share), F32),
            vm((2, 3, share, branch), F32),
            vm((both, depth), BF16),
            vm((tokens, depth), BF16),
            vm((both, depth), BF16),
            vm((both, depth), BF16),
            vm((both, tall), BF16),
            vm((tokens, branch), BF16),
            vm((tokens, wide), BF16),
            vm((2 * CHUNKS, chips, part, wide), F32),
            vm((4, 8, tokens), F32),
            vm((2 * CHUNKS, chips, part, wide), BF16),
            vm((CHUNKS, chips, part, wide), BF16),
            vm((2 * CHUNKS, chips, part, wide), BF16),
            vm((CHUNKS, chips, part, wide), BF16),
            vm((2 * CHUNKS, chips, part, wide), BF16),
            vm((2 * CHUNKS, part, wide), BF16),
            vm((CHUNKS, part, wide), BF16),
            vm((2 * CHUNKS, part, wide), BF16),
            vm((CHUNKS, part, wide), BF16),
            vm((2 * CHUNKS, part, wide), BF16),
            vm((CHUNKS, part, wide), BF16),
            vm((CHUNKS, part, wide), BF16),
            vm((CHUNKS, part, wide), BF16),
            many(SENDS + 7 * CHUNKS),
            many(42 * PIECES + (28 + 3 * SPLIT) * CHUNKS + 3),
            many(18),
        ],
        compiler_params=pltpu.CompilerParams(
            collective_id=0, has_side_effects=True, vmem_limit_bytes=67043328
        ),
    )
    return call(
        stream, first_gate, first_up, first_down, mixer_left, mixer_right, mixer_out,
        second_gate, second_up, second_down, flat(first_gain), flat(mixer_gain), flat(second_gain),
        first_gate_scale, first_up_scale, flat(first_down_scale), flat(mixer_left_scale),
        flat(mixer_right_scale), flat(mixer_out_scale), second_gate_scale, second_up_scale,
        flat(second_down_scale), flat(channel_gain), spatial, spatial_bias,
    )


def local(*args):
    if fits(args[0], args[2], args[9]):
        return fused(*args)
    return layer(*args)


def solution(mesh):
    return jax.shard_map(
        local,
        mesh=mesh,
        in_specs=(
            P("tp", ("grp", "fs")),
            P(),
            P("fs", "tp"),
            P("tp"),
            P("fs", "tp"),
            P("tp"),
            P("tp", "fs"),
            P("fs"),
            P(),
            P("fs", "tp"),
            P("tp"),
            P("fs", "tp"),
            P("tp"),
            P("tp"),
            P("tp", None, None),
            P("tp", None),
            P("tp", "fs"),
            P("fs"),
            P(),
            P("fs", "tp"),
            P("tp"),
            P("fs", "tp"),
            P("tp"),
            P("tp", "fs"),
            P("fs"),
        ),
        out_specs=P("tp", ("grp", "fs")),
        check_vma=False,
    )
```

```python
import jax
import jax.numpy as jnp
from jax import lax
from jax.experimental import pallas as pl
from jax.experimental.pallas import tpu as pltpu
from jax.sharding import PartitionSpec as P

EPS = 1e-06
CORES = 2
LANES = 128
CHUNKS = 3
PIECES = 2
SENDS = 32
AHEAD = (2, 2, 2, 2, 1, 2, 2, 2, 3, 2, 1, 4)
SPLIT = 1
MESH = pl.DeviceIdType.MESH
F32, BF16 = jnp.float32, jnp.bfloat16


def many(count):
    return pltpu.SemaphoreType.DMA((count,))


def kernel(
    stream, gate_1, up_1, down_1, left_w, right_w, out_w, gate_2, up_2, down_2,
    gain_1, gain_m, gain_2, gate_scale_1, up_scale_1, down_scale_1, left_scale, right_scale, out_scale,
    gate_scale_2, up_scale_2, down_scale_2, channel_gain, spatial, spatial_bias,
    result,
    weights, mixer_w, staged, turned, wide_in, tall_in, mixer_in,
    rows_1, rows_m, rows_2, normal, hidden, gated, held, kept, stats,
    core_out, core_out_m, core_in_1, core_in_m, core_in_2,
    chip_out, chip_out_m, chip_in_1, chip_in_m, chip_in_2,
    pair_out, pair_in_1, pair_in_2,
    send_sem, recv_sem, load_sem,
):
    grp, fs, tp = lax.axis_index("grp"), lax.axis_index("fs"), lax.axis_index("tp")
    groups, count, tps = lax.axis_size("grp"), lax.axis_size("fs"), lax.axis_size("tp")
    half = count // 2
    side = fs // half
    partner = lax.rem(fs + half, count)
    near = side * half + (1 - lax.rem(fs, half))
    core, chip = lax.rem(tp, CORES), tp // CORES
    sibling = chip * CORES + (1 - core)
    across = lax.rem(tp + CORES, tps)
    diagonal = lax.rem(sibling + CORES, tps)
    wide, tokens = stream.shape
    share = wide // groups
    tall = hidden.shape[1]
    part = tokens // CHUNKS
    branch = left_w.shape[1]

    to_partner, to_near = {"fs": partner}, {"fs": near}
    to_group = {"grp": 1 - grp}
    to_sibling, to_across, to_diagonal = {"tp": sibling}, {"tp": across}, {"tp": diagonal}
    every = (to_partner, to_near, to_group, to_sibling, to_across, to_diagonal)

    barrier = pltpu.get_barrier_semaphore()
    for device in every:
        pl.semaphore_signal(barrier, inc=1, device_id=device, device_id_type=MESH)

    used = [0, 0, SENDS]
    pending, taken, slots = [], [], list(range(SENDS))

    def send(source, target, device):
        if not slots:
            sent([pending[0]])
        slot = slots.pop(0)
        at = used[0]
        used[0] += 1
        copy = pltpu.make_async_remote_copy(
            src_ref=source,
            dst_ref=target,
            send_sem=send_sem.at[slot],
            recv_sem=recv_sem.at[at],
            device_id=device,
            device_id_type=MESH,
        )
        copy.start()
        pending.append(copy)
        taken.append(slot)
        return copy

    def reserve(source, target, device):
        at = used[0]
        used[0] += 1
        used[2] += 1
        return pltpu.make_async_remote_copy(
            src_ref=source,
            dst_ref=target,
            send_sem=send_sem.at[used[2] - 1],
            recv_sem=recv_sem.at[at],
            device_id=device,
            device_id_type=MESH,
        )

    def sent(copies):
        for copy in copies:
            for at, other in enumerate(pending):
                if other is copy:
                    copy.wait_send()
                    pending.pop(at)
                    slots.append(taken.pop(at))
                    break

    def load(source, target):
        at = used[1]
        used[1] += 1
        copy = pltpu.make_async_copy(source, target, load_sem.at[at])
        copy.start()
        return copy

    def place(source, member):
        return pl.ds(pl.multiple_of((source * groups + member) * share, share), share)

    def of_share(member):
        return pl.ds(pl.multiple_of(member * share, share), share)

    own_side = pl.ds(pl.multiple_of(side * tall, 16), tall)
    other_side = pl.ds(pl.multiple_of((1 - side) * tall, 16), tall)


    def load_rows(weight, member, slot):
        return load(weight.at[of_share(member), :], wide_in.at[slot])

    def load_cols(weight, member):
        return load(weight.at[:, of_share(member)], tall_in)

    def load_mixer(member, slot):
        return [
            load(left_w.at[of_share(member), :], mixer_in.at[slot, 0]),
            load(right_w.at[of_share(member), :], mixer_in.at[slot, 1]),
            load(out_w.at[:, of_share(member)], mixer_in.at[slot, 2]),
        ]

    def turn(slot, scale, target):
        def step(at, carry):
            lanes = pl.ds(pl.multiple_of(at * LANES, LANES), LANES)
            target[lanes, :] = (wide_in[slot, :, lanes] * scale[lanes][None, :]).T.astype(BF16)
            return carry

        lax.fori_loop(0, wide_in.shape[2] // LANES, step, 0)

    def cast_rows(unit, stage, slot, scale):
        target = turned if stage is None else staged.at[stage]
        turn(slot, scale, target)
        member = 1 - grp if stage is None else grp
        weights[unit, :, place(fs, member)] = target[own_side, :]

    def cast_cols(unit, stage, scale):
        member = 1 - grp if stage is None else grp
        factor = scale[:, of_share(member)]
        weights[unit, :, place(fs, member)] = (tall_in[own_side, :] * factor).astype(BF16)
        if stage is not None:
            staged[stage, 0:tall, :] = (tall_in[other_side, :] * factor).astype(BF16)

    def cast_mixer(slot, member):
        at = fs * groups + member
        mixer_w[at, 0:share, :] = (mixer_in[slot, 0] * left_scale[...]).astype(BF16)
        mixer_w[at, share : 2 * share, :] = (mixer_in[slot, 1] * right_scale[...]).astype(BF16)
        mixer_w[at, 2 * share : 3 * share, :] = (
            mixer_in[slot, 2] * out_scale[:, of_share(member)]
        ).astype(BF16)

    class Piece:
        def __init__(self, slot, source):
            self.slot, self.source = slot, source

        def begin(self):
            mine = self.slot(fs, grp)
            self.first = send(self.source() if self.source else mine, mine, to_partner)
            self.second = send(mine, mine, to_near)

        def relay_first(self):
            self.first.wait_recv()
            got = self.slot(partner, grp)
            self.swaps = [send(got, got, to_group)]
            self.third = send(got, got, to_near)

        def relay_second(self):
            self.second.wait_recv()
            got = self.slot(near, grp)
            self.swaps.append(send(got, got, to_group))

        def relay_third(self):
            self.third.wait_recv()
            got = self.slot(lax.rem(near + half, count), grp)
            self.swaps.append(send(got, got, to_group))

        def complete(self):
            for copy in self.swaps:
                copy.wait_recv()

    def hidden_pieces(unit, stage, turns, parts=PIECES):
        size = tall // parts

        def piece(at):
            first = at * size
            away = (1 - side) * tall + first if turns else first
            return Piece(
                lambda source, member: weights.at[unit, pl.ds(first, size), place(source, member)],
                lambda: staged.at[stage, pl.ds(pl.multiple_of(away, 16), size), :],
            )

        return [piece(at) for at in range(parts)]

    def mixer_pieces():
        size = mixer_w.shape[1] // PIECES

        def piece(at):
            rows = pl.ds(at * size, size)
            return Piece(lambda source, member: mixer_w.at[source * groups + member, rows, :], None)

        return [piece(at) for at in range(PIECES)]

    pieces = (
        hidden_pieces(0, 0, True) + hidden_pieces(1, 1, True) + hidden_pieces(2, 2, False) + mixer_pieces()
        + hidden_pieces(3, 0, True) + hidden_pieces(4, 1, True) + hidden_pieces(5, 2, False, 2 * PIECES)
    )

    begun_pieces = [2]

    def ahead(at):
        return AHEAD[min(at, len(AHEAD) - 1)]

    def pump(at):
        pieces[at].relay_first()
        pieces[at].relay_second()
        for following in range(begun_pieces[0], min(at + ahead(at), len(pieces) - 1) + 1):
            pieces[following].begin()
            begun_pieces[0] += 1

    def third(at):
        pieces[at].relay_third()

    def complete(first, last):
        for piece in pieces[first * PIECES : last * PIECES]:
            piece.complete()


    def gather_begin(rows, pair):
        def view(at_side, at_tp, at):
            first = at_side * tokens + at * part if pair else at * part
            return rows.at[
                pl.ds(pl.multiple_of(first, part), part),
                pl.ds(pl.multiple_of(at_tp * wide, wide), wide),
            ]

        chips, cores = [], []
        for at in range(CHUNKS):
            mine = view(side, tp, at)
            chips.append(send(mine, mine, to_across))
            cores.append(send(mine, mine, to_sibling))
        return view, [], chips, cores

    def gather_pair(begun):
        view, firsts, _, _ = begun
        size = wide // SPLIT
        for at in range(CHUNKS):
            mine = view(side, tp, at)
            narrow = [mine.at[:, first * size : (first + 1) * size] for first in range(SPLIT)]
            firsts.append([send(block, block, to_partner) for block in narrow])

    def relay_own(begun):
        view, _, chips, cores = begun
        for at in range(CHUNKS):
            chips[at].wait_recv()
            got = view(side, across, at)
            cores.append(send(got, got, to_sibling))

    def relay_pair(begun):
        view, firsts, _, _ = begun
        seconds, cores = [], []
        for at in range(CHUNKS):
            for copy in firsts[at]:
                copy.wait_recv()
            got = view(1 - side, tp, at)
            seconds.append(send(got, got, to_across))
            cores.append(send(got, got, to_sibling))
        return seconds, cores

    def end_own(begun):
        for copy in begun[3]:
            copy.wait_recv()

    def end_pair(begun, relayed):
        view = begun[0]
        seconds, cores = relayed
        for at, copy in enumerate(seconds):
            copy.wait_recv()
            got = view(1 - side, across, at)
            cores.append(send(got, got, to_sibling))
        for copy in cores:
            copy.wait_recv()

    def own_rows(rows, pair):
        first = pl.multiple_of(side * tokens, part) if pair else 0
        rows[pl.ds(first, tokens), pl.ds(pl.multiple_of(tp * wide, wide), wide)] = held[...]

    def norm(rows, gain, first):
        size = 64

        def step(at, carry):
            here = pl.ds(pl.multiple_of(first + at * size, size), size)
            values = rows[here, :].astype(F32)
            inverse = lax.rsqrt(jnp.mean(values * values, axis=1, keepdims=True) + EPS)
            normal[here, :] = (values * inverse * gain[...]).astype(BF16)
            return carry

        lax.fori_loop(0, tokens // size, step, 0)

    def expand(unit, between=None):
        def step(at):
            here = pl.ds(at * tokens, tokens)
            values = normal[here, :]
            dims = (((1,), (1,)), ((), ()))
            gate = lax.dot_general(values, weights[unit], dims, preferred_element_type=F32)
            upward = lax.dot_general(values, weights[unit + 1], dims, preferred_element_type=F32)
            hidden[here, :] = (gate / (1.0 + jnp.exp(-gate)) * upward).astype(BF16)

        step(0)
        if between is not None:
            between()
        step(1)

    def reduce_sums(tiles, product, outs, ins, between):
        core_to, chip_to, pair_to = outs
        core_from, chip_from, pair_from = ins
        firsts, seconds, thirds = {}, {}, {}
        size = wide // SPLIT
        halves = [slice(at * size, (at + 1) * size) for at in range(SPLIT)]

        def begin(at):
            for to_chip in range(tps // CORES):
                other = to_chip * CORES + 1 - core
                core_to[at, to_chip] = product(tiles[at][0], other).astype(BF16)
            firsts[at] = send(core_to.at[at], core_from.at[at], to_sibling)
            for to_chip in range(tps // CORES):
                kept[at, to_chip] = product(tiles[at][0], to_chip * CORES + core)

        def chips(at):
            firsts[at].wait_recv()
            away = 1 - chip
            chip_to[at] = (kept[at, away] + core_from[at, away].astype(F32)).astype(BF16)
            seconds[at] = send(chip_to.at[at], chip_from.at[at], to_across)
            kept[at, chip] = kept[at, chip] + core_from[at, chip].astype(F32)

        def pairs(at):
            seconds[at].wait_recv()
            total = kept[at, chip] + chip_from[at].astype(F32)
            if tiles[at][1]:
                pair_to[at] = total.astype(BF16)
                thirds[at] = [
                    send(pair_to.at[at, :, columns], pair_from.at[at, :, columns], to_partner)
                    for columns in halves
                ]
            else:
                kept[at, chip] = total

        for at in range(len(tiles) + 2):
            if at < len(tiles):
                begin(at)
            if 0 <= at - 1 < len(tiles):
                chips(at - 1)
            if 0 <= at - 2 < len(tiles):
                pairs(at - 2)
            between(at)
        own = [at for at in range(len(tiles)) if not tiles[at][1]]
        for order, at in enumerate(own):
            total = kept[at, chip]
            if thirds:
                for copy in thirds[order]:
                    copy.wait_recv()
                total = total + pair_from[order].astype(F32)
            here = pl.ds(order * part, part)
            factor = 0.5 if thirds else 1.0
            held[here, :] = (held[here, :].astype(F32) + factor * total).astype(BF16)
        return list(firsts.values()) + list(seconds.values()) + sum(thirds.values(), [])

    def half_tiles():
        away = [((1 - side) * tokens + at * part, True) for at in range(CHUNKS)]
        return away + [(side * tokens + at * part, False) for at in range(CHUNKS)]

    def down_product(unit):
        def product(first, target):
            values = hidden[pl.ds(pl.multiple_of(first, part), part), :]
            columns = pl.ds(pl.multiple_of(target * wide, wide), wide)
            return jnp.dot(values, weights[unit, :, columns], preferred_element_type=F32)

        return product

    class Targets:
        def __init__(self, tiles, product):
            self.tiles, self.product = tiles, product
            self.order = (fs, partner, near, lax.rem(near + half, count))
            self.cores = [
                reserve(core_out.at[at, step], core_in_2.at[at, step], to_sibling)
                for step in range(2)
                for at in range(len(tiles))
            ]
            self.chips = [reserve(chip_out.at[at], chip_in_2.at[at], to_across) for at in range(len(tiles))]
            self.pairs = [reserve(pair_out.at[at], pair_in_2.at[at], to_partner) for at in range(CHUNKS)]

        def roles(self, step):
            target = self.order[step]
            hold = lax.rem(target, CORES) == core
            here = target // CORES == chip
            return target, hold, here

        def begin(self, step, pair):
            target, hold, here = self.roles(step)
            size = len(self.tiles)
            chosen = [at for at in range(size) if self.tiles[at][1] == pair]

            def product(at):
                value = self.product(self.tiles[at][0], target)

                @pl.when(jnp.logical_not(hold))
                def _():
                    core_out[at, step % 2] = value.astype(BF16)
                    self.cores[step % 2 * size + at].start()

                @pl.when(hold)
                def _():
                    kept[at, here.astype(jnp.int32)] = value

            def add(at):
                @pl.when(hold)
                def _():
                    self.cores[step % 2 * size + at].wait_recv()
                    slot = here.astype(jnp.int32)
                    value = kept[at, slot] + core_in_2[at, step % 2].astype(F32)

                    @pl.when(here)
                    def _():
                        kept[at, 1] = value

                    @pl.when(jnp.logical_not(here))
                    def _():
                        chip_out[at] = value.astype(BF16)
                        self.chips[at].start()

            for order in range(len(chosen) + 1):
                if order < len(chosen):
                    product(chosen[order])
                if order > 0:
                    add(chosen[order - 1])

        def end(self, step, pair):
            _, hold, here = self.roles(step)
            chosen = [at for at in range(len(self.tiles)) if self.tiles[at][1] == pair]

            @pl.when(jnp.logical_and(hold, here))
            def _():
                for at in chosen:
                    self.chips[at].wait_recv()
                    value = kept[at, 1] + chip_in_2[at].astype(F32)
                    if self.tiles[at][1]:
                        pair_out[at] = value.astype(BF16)
                        self.pairs[at].start()
                    else:
                        kept[at, 1] = value

        def finish(self):
            own = [at for at in range(len(self.tiles)) if not self.tiles[at][1]]
            for order, at in enumerate(own):
                self.pairs[order].wait_recv()
                total = kept[at, 1] + pair_in_2[order].astype(F32)
                here = pl.ds(order * part, part)
                held[here, :] = (held[here, :].astype(F32) + 0.5 * total).astype(BF16)

        def drain(self):
            size = len(self.tiles)
            for step in range(len(self.order)):
                _, hold, here = self.roles(step)

                @pl.when(jnp.logical_not(hold))
                def _(step=step):
                    for at in range(size):
                        self.cores[step % 2 * size + at].wait_send()

                @pl.when(jnp.logical_and(hold, jnp.logical_not(here)))
                def _(step=step):
                    for at in range(size):
                        self.chips[at].wait_send()

            for copy in self.pairs:
                copy.wait_send()


    loads = {"g1": load_rows(gate_1, grp, 0), "u1": load_rows(up_1, grp, 1), "d1": load_cols(down_1, grp)}
    held[...] = stream[...].astype(F32).T.astype(BF16)
    own_rows(rows_1, True)
    loads["g1"].wait()
    cast_rows(0, 0, 0, gate_scale_1)
    loads["g1"] = load_rows(gate_1, 1 - grp, 0)
    pl.semaphore_wait(barrier, len(every))
    pieces[0].begin()
    pieces[1].begin()
    begun = gather_begin(rows_1, True)
    loads["u1"].wait()
    cast_rows(1, 1, 1, up_scale_1)
    loads["u1"] = load_rows(up_1, 1 - grp, 1)
    loads["d1"].wait()
    cast_cols(2, 2, down_scale_1)
    loads["d1"] = load_cols(down_1, 1 - grp)
    loads["m"] = load_mixer(grp, 0)
    loads["n"] = load_mixer(1 - grp, 1)
    loads["g1"].wait()
    cast_rows(0, None, 0, gate_scale_1)
    loads["g2"] = load_rows(gate_2, grp, 0)
    pump(0)
    loads["u1"].wait()
    cast_rows(1, None, 1, up_scale_1)
    loads["u2"] = load_rows(up_2, grp, 1)
    pump(1)
    loads["d1"].wait()
    cast_cols(2, None, down_scale_1)
    loads["d2"] = load_cols(down_2, grp)
    for copy in loads["m"] + loads["n"]:
        copy.wait()
    cast_mixer(0, grp)
    cast_mixer(1, 1 - grp)
    third(0)
    gather_pair(begun)
    pump(2)
    sent([piece.first for piece in pieces[0:2]])
    loads["g2"].wait()
    cast_rows(3, 0, 0, gate_scale_2)
    loads["g2"] = load_rows(gate_2, 1 - grp, 0)
    third(1)
    pump(3)
    relay_own(begun)
    relayed = relay_pair(begun)
    third(2)
    sent([piece.first for piece in pieces[2:4]])
    loads["u2"].wait()
    cast_rows(4, 1, 1, up_scale_2)
    loads["u2"] = load_rows(up_2, 1 - grp, 1)
    pump(4)
    end_own(begun)
    end_pair(begun, relayed)
    norm(rows_1, gain_1, 0)
    norm(rows_1, gain_1, tokens)
    third(3)
    loads["g2"].wait()
    cast_rows(3, None, 0, gate_scale_2)
    pump(5)
    sent([piece.first for piece in pieces[4:6]])
    loads["d2"].wait()
    cast_cols(5, 2, down_scale_2)
    loads["d2"] = load_cols(down_2, 1 - grp)
    third(4)
    loads["u2"].wait()
    cast_rows(4, None, 1, up_scale_2)
    loads["d2"].wait()
    cast_cols(5, None, down_scale_2)
    complete(0, 2)
    expand(0)
    third(5)
    complete(2, 3)

    def between_1(at):
        if at == 0:
            pump(6)
        if at == 3:
            third(6)
        if at == 5:
            pump(7)
        if at == 7:
            third(7)

    copies = reduce_sums(
        half_tiles(), down_product(2), (core_out, chip_out, pair_out),
        (core_in_1, chip_in_1, pair_in_1), between_1,
    )

    own_rows(rows_m, False)
    begun = gather_begin(rows_m, False)
    relay_own(begun)
    pump(8)
    end_own(begun)
    norm(rows_m, gain_m, 0)
    complete(3, 4)

    def projection(first):
        total = None
        for at in range(count * groups):
            term = jnp.dot(
                normal[0:tokens, at * share : (at + 1) * share],
                mixer_w[at, first : first + share, :],
                preferred_element_type=F32,
            )
            total = term if total is None else total + term
        return jax.nn.gelu(total)

    right = projection(share)
    lane = lax.broadcasted_iota(jnp.int32, (tokens, LANES), 1)
    summed = jnp.sum(right, axis=1, keepdims=True)
    squares = jnp.sum(right * right, axis=1, keepdims=True)
    packed = jnp.where(lane == 0, summed, jnp.where(lane == 1, squares, 0.0))
    stats[0] = packed.T[0:8, :]
    shared = [
        send(stats.at[0], stats.at[1], to_sibling),
        send(stats.at[0], stats.at[2], to_across),
        send(stats.at[0], stats.at[3], to_diagonal),
    ]
    left = projection(0)
    for copy in shared:
        copy.wait_recv()
    total = (stats[0] + stats[1]) + (stats[2] + stats[3])
    total = jnp.concatenate([total, jnp.zeros((LANES - 8, tokens), F32)], axis=0).T
    size = branch * tps
    average = total[:, 0:1] / size
    inverse = lax.rsqrt(total[:, 1:2] / size - average * average + EPS)
    centred = ((right - average) * inverse * channel_gain[...]).astype(BF16)
    span = spatial.shape[1]
    rest = jnp.zeros((span - spatial_bias.shape[0], span), F32)
    bias = jnp.concatenate([spatial_bias[...], rest], axis=0).T
    target = lax.broadcasted_iota(jnp.int32, (span, span), 0)
    source = lax.broadcasted_iota(jnp.int32, (span, span), 1)
    members = branch // spatial.shape[0]
    for group in range(spatial.shape[0]):
        matrix = jnp.where(source <= target, spatial[group].astype(F32), 0.0).astype(BF16)
        columns = slice(group * members, (group + 1) * members)
        for at in range(tokens // span):
            here = slice(at * span, (at + 1) * span)
            mixed = jnp.dot(matrix, centred[here, columns], preferred_element_type=F32)
            mixed = mixed + bias[:, group : group + 1]
            gated[here, columns] = (left[here, columns] * mixed).astype(BF16)

    def out_product(first, target):
        values = gated[first : first + part, :]
        each = wide // share
        return jnp.concatenate(
            [
                jnp.dot(
                    values,
                    mixer_w[target * each + at, 2 * share : 3 * share, :],
                    preferred_element_type=F32,
                )
                for at in range(each)
            ],
            axis=1,
        )

    def between_m(at):
        if at == 1:
            third(8)
            pump(9)
        if at == 4:
            pump(10)

    reduce_sums(
        [(at * part, False) for at in range(CHUNKS)], out_product, (core_out_m, chip_out_m, None),
        (core_in_m, chip_in_m, None), between_m,
    )

    own_rows(rows_2, True)
    begun = gather_begin(rows_2, True)
    gather_pair(begun)
    third(9)
    pump(11)
    relay_own(begun)
    third(10)
    relayed = relay_pair(begun)
    end_own(begun)
    norm(rows_2, gain_2, side * tokens)
    third(11)
    pump(12)
    end_pair(begun, relayed)
    norm(rows_2, gain_2, (1 - side) * tokens)
    pump(13)
    complete(4, 6)
    pump(14)
    expand(3, lambda: pump(15))
    sent(copies)
    sums = Targets(half_tiles(), down_product(5))
    last = pieces[6 * PIECES :]

    def arrived(step):
        for piece in last:
            piece.swaps[step].wait_recv()

    third(12)
    third(13)
    sums.begin(0, True)
    sums.begin(0, False)
    arrived(0)
    third(14)
    third(15)
    sums.begin(1, True)
    sums.begin(1, False)
    arrived(1)
    sums.begin(2, True)
    sums.end(0, True)
    sums.end(1, True)
    arrived(2)
    sums.begin(3, True)
    sums.end(2, True)
    sums.end(3, True)
    sums.begin(2, False)
    sums.begin(3, False)
    for step in range(count):
        sums.end(step, False)
    sums.finish()
    result[...] = held[...].astype(F32).T.astype(BF16)
    sent(list(pending))
    sums.drain()


def contract(left_side, right_side):
    return lax.dot_general(
        left_side, right_side, (((0,), (0,)), ((), ())), preferred_element_type=jnp.float32
    )


def product(left_side, right_side):
    return lax.dot_general(
        left_side, right_side, (((1,), (0,)), ((), ())), preferred_element_type=jnp.float32
    )


def permuted(block, axis_name, target):
    count = lax.axis_size(axis_name)
    return lax.ppermute(block, axis_name, [(at, target(at, count)) for at in range(count)])


def to_partner(block):
    return permuted(block, "fs", lambda at, count: (at + count // 2) % count)


def in_half(block, step):
    def target(at, count):
        half = count // 2
        return at // half * half + (at % half + step) % half

    return permuted(block, "fs", target)


def to_other_grp(block, step):
    return permuted(block, "grp", lambda at, count: (at + step) % count)


def to_same_core(block, step):
    return permuted(block, "tp", lambda at, count: (at + step * CORES) % count)


def to_other_core(block):
    return permuted(block, "tp", lambda at, count: at ^ 1)


def pick(blocks, index):
    count = len(blocks)
    if count == 1:
        return blocks[0]
    index = lax.rem(index + count, count)
    found = blocks[0]
    for at in range(1, count):
        found = jnp.where(index == at, blocks[at], found)
    return found


def chip_and_core():
    place = lax.axis_index("tp")
    return lax.div(place, CORES), lax.rem(place, CORES)


def gather_rows(block):
    chips = lax.axis_size("tp") // CORES
    chip, core = chip_and_core()
    held = jnp.stack([block] + [to_same_core(block, step) for step in range(1, chips)])
    other = to_other_core(held)
    found = []
    for at_chip in range(chips):
        mine = pick([held[step] for step in range(chips)], chip - at_chip)
        theirs = pick([other[step] for step in range(chips)], chip - at_chip)
        found += [jnp.where(core == 0, mine, theirs), jnp.where(core == 0, theirs, mine)]
    return jnp.concatenate(found)


def scatter_sum(terms):
    chips = lax.axis_size("tp") // CORES
    chip, core = chip_and_core()
    blocks = terms.reshape((chips, CORES, -1) + terms.shape[1:])
    mine = jnp.where(core == 0, blocks[:, 0], blocks[:, 1])
    passed = jnp.where(core == 0, blocks[:, 1], blocks[:, 0])
    pairs = mine.astype(jnp.float32) + to_other_core(passed).astype(jnp.float32)
    total = pick([pairs[at] for at in range(chips)], chip)
    for step in range(1, chips):
        sent = pick([pairs[at] for at in range(chips)], chip + step).astype(jnp.bfloat16)
        total = total + to_same_core(sent, step).astype(jnp.float32)
    return total


def places():
    count = lax.axis_size("fs")
    half = count // 2
    me = lax.axis_index("fs")
    low = lax.rem(me, half)
    found = []
    for step in range(half):
        near = me - low + lax.rem(low - step + half, half)
        found += [near, lax.rem(near + half, count)]
    return found


def shares():
    count = lax.axis_size("grp")
    me = lax.axis_index("grp")
    return [lax.rem(me - back + count, count) for back in range(count)]


def gathered(kept, passed, others):
    half = lax.axis_size("fs") // 2
    got = to_partner(passed)
    mine = [kept, got]
    for step in range(1, half):
        mine += [in_half(kept, step), in_half(got, step)]
    found = [mine]
    for back, own in zip(range(1, lax.axis_size("grp")), others):
        found.append([own] + [to_other_grp(block, back) for block in mine[1:]])
    return found


def rows_unit(weights):
    half = lax.div(lax.axis_index("fs"), lax.axis_size("fs") // 2)

    def cut(index, side):
        found = []
        for weight in weights:
            width = weight.shape[0] // lax.axis_size("grp")
            wide = weight.shape[1] // 2
            part = lax.dynamic_slice(weight, (index * width, side * wide), (width, wide))
            found.append(part.astype(jnp.bfloat16).T)
        return jnp.stack(found)

    order = shares()
    return gathered(
        cut(order[0], half), cut(order[0], 1 - half), [cut(index, half) for index in order[1:]]
    )


def cols_unit(weight):
    half = lax.div(lax.axis_index("fs"), lax.axis_size("fs") // 2)

    def cut(index, side):
        width = weight.shape[1] // lax.axis_size("grp")
        tall = weight.shape[0] // 2
        part = lax.dynamic_slice(weight, (side * tall, index * width), (tall, width))
        return part.astype(jnp.bfloat16)

    order = shares()
    return gathered(
        cut(order[0], half), cut(order[0], 1 - half), [cut(index, half) for index in order[1:]]
    )


def mixer_unit(left, right, out):
    def cut(index):
        width = left.shape[0] // lax.axis_size("grp")
        rows = [
            lax.dynamic_slice_in_dim(weight, index * width, width, 0).astype(jnp.bfloat16).T
            for weight in (left, right)
        ]
        return jnp.stack(rows + [lax.dynamic_slice_in_dim(out, index * width, width, 1).astype(jnp.bfloat16)])

    order = shares()
    share = cut(order[0])
    return gathered(share, share, [cut(index) for index in order[1:]])


def rows_in_order(rows):
    count, groups = lax.axis_size("fs"), lax.axis_size("grp")
    width = rows.shape[0] // (count * groups)
    pieces = []
    for share in shares():
        for place in places():
            pieces.append(
                lax.dynamic_slice_in_dim(rows, (place * groups + share) * width, width, 0)
            )
    return jnp.concatenate(pieces)


def joined(blocks):
    return jnp.concatenate([block for mine in blocks for block in mine], axis=-1)


def columns_out(blocks, hidden):
    count, groups = lax.axis_size("fs"), lax.axis_size("grp")
    every = joined(blocks)
    width = every.shape[1] // (count * groups)
    terms = contract(every, hidden).astype(jnp.bfloat16)
    found = jnp.zeros_like(terms)
    at = 0
    for share in shares():
        for place in places():
            found = lax.dynamic_update_slice_in_dim(
                found, terms[at : at + width], (place * groups + share) * width, 0
            )
            at += width
    return found


def inverse_of(values):
    return lax.rsqrt(jnp.mean(values * values, axis=0) + EPS)


def normed(whole_rows, gain):
    values = whole_rows.astype(jnp.float32)
    return (values * inverse_of(values) * gain[:, None]).astype(jnp.bfloat16)


def half_step(stream, gain, rows_blocks, gate_scale, up_scale, cols_blocks, down_scale):
    tokens = stream.shape[1]
    both = jnp.concatenate([stream, to_partner(stream)], axis=1)
    rows = rows_in_order(normed(gather_rows(both), gain))
    half = lax.div(lax.axis_index("fs"), lax.axis_size("fs") // 2)
    tall = gate_scale.shape[0] // 2
    gate_scale = lax.dynamic_slice_in_dim(gate_scale, half * tall, tall)[:, None]
    up_scale = lax.dynamic_slice_in_dim(up_scale, half * tall, tall)[:, None]
    every = joined(rows_blocks)
    gate = product(every[0], rows)
    upward = product(every[1], rows)
    hidden = (jax.nn.silu(gate * gate_scale) * (upward * up_scale)).astype(jnp.bfloat16)
    total = scatter_sum(columns_out(cols_blocks, hidden))
    away = to_partner(total[:, tokens:].astype(jnp.bfloat16))
    total = total[:, :tokens] + away.astype(jnp.float32)
    return (stream.astype(jnp.float32) + 0.5 * (total * down_scale[:, None])).astype(jnp.bfloat16)


def gating_unit(left_pre, right_pre, channel_gain, spatial, spatial_bias):
    left = jax.nn.gelu(left_pre)
    right = jax.nn.gelu(right_pre)
    branch = channel_gain.shape[0] * lax.axis_size("tp")
    totals, squares = lax.psum((jnp.sum(right, axis=0), jnp.sum(right * right, axis=0)), "tp")
    average = totals / branch
    inverse = lax.rsqrt(squares / branch - average * average + EPS)
    centred = ((right - average) * inverse * channel_gain[:, None]).astype(jnp.bfloat16)
    local_groups, span = (spatial.shape[0], spatial.shape[1])
    tokens = centred.shape[1]
    blocks = centred.reshape(local_groups, centred.shape[0] // local_groups, tokens // span, span)
    target = lax.broadcasted_iota(jnp.int32, (span, span), 0)
    source = lax.broadcasted_iota(jnp.int32, (span, span), 1)
    masked = jnp.where((source <= target)[None], spatial, jnp.zeros_like(spatial))
    token_mix = jnp.einsum("gts,gcns->gcnt", masked, blocks, preferred_element_type=jnp.float32)
    token_mix = token_mix + spatial_bias[:, None, None, :]
    return (left * token_mix.reshape(centred.shape[0], tokens)).astype(jnp.bfloat16)


def layer(
    stream,
    first_gain,
    first_gate,
    first_gate_scale,
    first_up,
    first_up_scale,
    first_down,
    first_down_scale,
    mixer_gain,
    mixer_left,
    mixer_left_scale,
    mixer_right,
    mixer_right_scale,
    channel_gain,
    spatial,
    spatial_bias,
    mixer_out,
    mixer_out_scale,
    second_gain,
    second_gate,
    second_gate_scale,
    second_up,
    second_up_scale,
    second_down,
    second_down_scale,
):
    held = jnp.stack([first_down_scale, mixer_out_scale, second_down_scale])
    count = lax.axis_size("fs")
    me = lax.axis_index("fs")
    parts = [held] + [
        permuted(held, "fs", lambda at, count, step=step: (at + step) % count)
        for step in range(1, count)
    ]
    scales = jnp.concatenate([pick(parts, me - place) for place in range(count)], axis=1)
    wide = stream.shape[0]
    scales = lax.dynamic_slice_in_dim(scales, lax.axis_index("tp") * wide, wide, 1)

    first_rows = rows_unit((first_gate, first_up))
    first_cols = cols_unit(first_down)
    mixer = mixer_unit(mixer_left, mixer_right, mixer_out)
    second_rows = rows_unit((second_gate, second_up))
    second_cols = cols_unit(second_down)

    stream = half_step(
        stream, first_gain, first_rows, first_gate_scale, first_up_scale, first_cols, scales[0]
    )
    rows = rows_in_order(normed(gather_rows(stream), mixer_gain))
    lefts = joined([[block[0] for block in mine] for mine in mixer])
    rights = joined([[block[1] for block in mine] for mine in mixer])
    gated = gating_unit(
        product(lefts, rows) * mixer_left_scale[:, None],
        product(rights, rows) * mixer_right_scale[:, None],
        channel_gain,
        spatial,
        spatial_bias,
    )
    total = scatter_sum(columns_out([[block[2] for block in mine] for mine in mixer], gated))
    stream = (stream.astype(jnp.float32) + total * scales[1][:, None]).astype(jnp.bfloat16)
    return half_step(
        stream, second_gain, second_rows, second_gate_scale, second_up_scale, second_cols, scales[2]
    )


def fits(stream, first_gate, mixer_left):
    groups, count, tps = lax.axis_size("grp"), lax.axis_size("fs"), lax.axis_size("tp")
    share = stream.shape[0] // groups
    tall = first_gate.shape[1] // 2
    return (
        groups == 2
        and count == 4
        and count == tps
        and tps == 2 * CORES
        and first_gate.shape[0] == stream.shape[0]
        and share % LANES == 0
        and mixer_left.shape[1] == share
        and tall % 16 == 0
        and (2 * tall) % LANES == 0
        and stream.shape[0] % (LANES * SPLIT) == 0
        and stream.shape[1] % (LANES * CHUNKS) == 0
        and tall % (32 * PIECES) == 0
    )


def fused(
    stream, first_gain, first_gate, first_gate_scale, first_up, first_up_scale, first_down, first_down_scale,
    mixer_gain, mixer_left, mixer_left_scale, mixer_right, mixer_right_scale, channel_gain, spatial,
    spatial_bias, mixer_out, mixer_out_scale, second_gain, second_gate, second_gate_scale, second_up,
    second_up_scale, second_down, second_down_scale,
):
    def flat(vector):
        return vector.reshape(1, -1)

    groups, count, tps = lax.axis_size("grp"), lax.axis_size("fs"), lax.axis_size("tp")
    wide, tokens = stream.shape
    share, tall, depth = wide // groups, first_gate.shape[1] // 2, wide * tps
    branch, part = mixer_left.shape[1], tokens // CHUNKS
    both = 2 * tokens
    any_spec, vmem = pl.BlockSpec(memory_space=pl.ANY), pl.BlockSpec(memory_space=pltpu.VMEM)
    chips = tps // CORES
    vm = pltpu.VMEM
    call = pl.pallas_call(
        kernel,
        out_shape=jax.ShapeDtypeStruct((wide, tokens), BF16),
        in_specs=[vmem] + [any_spec] * 9 + [vmem] * 15,
        out_specs=vmem,
        scratch_shapes=[
            vm((6, tall, depth), BF16),
            vm((count * groups, 3 * share, branch), BF16),
            vm((3, 2 * tall, share), BF16),
            vm((2 * tall, share), BF16),
            vm((2, share, 2 * tall), F32),
            vm((2 * tall, share), F32),
            vm((2, 3, share, branch), F32),
            vm((both, depth), BF16),
            vm((tokens, depth), BF16),
            vm((both, depth), BF16),
            vm((both, depth), BF16),
            vm((both, tall), BF16),
            vm((tokens, branch), BF16),
            vm((tokens, wide), BF16),
            vm((2 * CHUNKS, chips, part, wide), F32),
            vm((4, 8, tokens), F32),
            vm((2 * CHUNKS, chips, part, wide), BF16),
            vm((CHUNKS, chips, part, wide), BF16),
            vm((2 * CHUNKS, chips, part, wide), BF16),
            vm((CHUNKS, chips, part, wide), BF16),
            vm((2 * CHUNKS, chips, part, wide), BF16),
            vm((2 * CHUNKS, part, wide), BF16),
            vm((CHUNKS, part, wide), BF16),
            vm((2 * CHUNKS, part, wide), BF16),
            vm((CHUNKS, part, wide), BF16),
            vm((2 * CHUNKS, part, wide), BF16),
            vm((CHUNKS, part, wide), BF16),
            vm((CHUNKS, part, wide), BF16),
            vm((CHUNKS, part, wide), BF16),
            many(SENDS + 7 * CHUNKS),
            many(48 * PIECES + (28 + 3 * SPLIT) * CHUNKS + 3),
            many(18),
        ],
        compiler_params=pltpu.CompilerParams(
            collective_id=0, has_side_effects=True, vmem_limit_bytes=67043328
        ),
    )
    return call(
        stream, first_gate, first_up, first_down, mixer_left, mixer_right, mixer_out,
        second_gate, second_up, second_down, flat(first_gain), flat(mixer_gain), flat(second_gain),
        first_gate_scale, first_up_scale, flat(first_down_scale), flat(mixer_left_scale),
        flat(mixer_right_scale), flat(mixer_out_scale), second_gate_scale, second_up_scale,
        flat(second_down_scale), flat(channel_gain), spatial, spatial_bias,
    )


def local(*args):
    if fits(args[0], args[2], args[9]):
        return fused(*args)
    return layer(*args)


def solution(mesh):
    return jax.shard_map(
        local,
        mesh=mesh,
        in_specs=(
            P("tp", ("grp", "fs")),
            P(),
            P("fs", "tp"),
            P("tp"),
            P("fs", "tp"),
            P("tp"),
            P("tp", "fs"),
            P("fs"),
            P(),
            P("fs", "tp"),
            P("tp"),
            P("fs", "tp"),
            P("tp"),
            P("tp"),
            P("tp", None, None),
            P("tp", None),
            P("tp", "fs"),
            P("fs"),
            P(),
            P("fs", "tp"),
            P("tp"),
            P("fs", "tp"),
            P("tp"),
            P("tp", "fs"),
            P("fs"),
        ),
        out_specs=P("tp", ("grp", "fs")),
        check_vma=False,
    )
```
